256 devices in a mesh: sp: 16 (over y, x), tp: 16 (over z, core).
Axes of the slice: x: 4, y: 4, z: 8, core: 2. Of those that a mesh axis runs over, the one named last changes fastest.
Arguments:
- queries: bfloat16 [32768, 2048], P('sp', 'tp'), may hold values from -160 to 160
- key_heads: bfloat16 [32768, 512], P('sp'), may hold values from -8 to 8
- value_heads: bfloat16 [32768, 512], P('sp'), may hold values from -4 to 4
- sink_logit: float32 [16], P('tp'), may hold values from -2 to 7
- out_weight: bfloat16 [2048, 2048], P('tp'), may hold values from -0.125 to 0.125
- residual: bfloat16 [32768, 2048], P(('sp', 'tp')), may hold values from -6 to 6
- mixer_gain: float32 [2048], replicated, may hold values from 0.1 to 1.9
- expert_gain: float32 [2048], replicated, may hold values from 0.1 to 1.9
- route_group: int32 [32768], P(('sp', 'tp')), may hold values from 0 to 15, as said below
- route_member: int32 [32768, 2], P(('sp', 'tp')), may hold values from 0 to 2, as said below
- route_weight: bfloat16 [32768, 2], P(('sp', 'tp')), may hold values from 0.19921875 to 1
- gate_weight: bfloat16 [48, 2048, 2048], P('sp', None, 'tp'), may hold values from -0.125 to 0.125
- up_weight: bfloat16 [48, 2048, 2048], P('sp', None, 'tp'), may hold values from -0.125 to 0.125
- down_weight: bfloat16 [48, 2048, 2048], P('sp', 'tp'), may hold values from -0.125 to 0.125
Outputs:
- output: bfloat16 [32768, 2048], P(('sp', 'tp'))
The draws below stay inside these ranges and needn't reach their ends.
Inputs may be any that keep to these rules, and one draw needn't show every extreme that they name: `route_group`: among the tokens of one device, at most 10 name one group; in every draw one group is named by exactly 10 tokens of every device. `route_member`: the two entries of a token are different members of its group.
All inputs are finite; a program needn't handle non-finite values.
Results may differ from the reference program's by a relative error of at most 0.018.
Values may be sent and summed in bfloat16 or wider, within the bound.
No kernel may reach another device: no remote copies, remote signals or barrier semaphores. Data moves between devices by JAX's collectives and lax.ppermute only.
A program may use at most 128 MiB of HBM per device.

```python
import jax
import jax.numpy as jnp
from jax import lax

D = 2048
HEADS = 16
KV_HEADS = 4
HEAD_DIM = 128
WINDOW = 128
BLOCK = 128
EXP_HID = 2048
GROUP_EXPERTS = 3
TOP = 2
TOK_DEV = 128
TOKENS = 32768
GROUPS = 16
EXPERTS = 48
GROUP_CAP = 10
N_TP = 16


def draw_key_heads(key, part):
    return jnp.clip(jax.random.normal(jax.random.fold_in(key, 37), (TOKENS, KV_HEADS * HEAD_DIM), jnp.float32), -4.0, 4.0).astype(jnp.bfloat16)


def draw_queries(key, part):
    drawn_rows = jnp.clip(jax.random.normal(jax.random.fold_in(key, 41), (TOKENS, HEADS * HEAD_DIM), jnp.float32), -4.0, 4.0)
    return drawn_rows.astype(jnp.bfloat16)


def route_table(key):
    base_key = jax.random.fold_in(key, 53)
    blocks = TOKENS // TOK_DEV
    slot_count = GROUPS * GROUP_CAP
    favored = jax.random.randint(jax.random.fold_in(base_key, 1), (), 0, GROUPS)

    def one_block(block_key):
        slot_order = jax.random.permutation(jax.random.fold_in(block_key, 1), slot_count)
        ranking = jnp.where(slot_order // GROUP_CAP == favored, 0, 1) * slot_count + jnp.arange(slot_count, dtype=jnp.int32)
        taken_slots = slot_order[jnp.argsort(ranking)][:TOK_DEV]
        shuffled = taken_slots[jax.random.permutation(jax.random.fold_in(block_key, 2), TOK_DEV)]
        chosen = shuffled // GROUP_CAP
        first_member = jax.random.randint(jax.random.fold_in(block_key, 3), (TOK_DEV,), 0, GROUP_EXPERTS)
        stepping = jax.random.randint(jax.random.fold_in(block_key, 4), (TOK_DEV,), 1, GROUP_EXPERTS)
        second = (first_member + stepping) % GROUP_EXPERTS
        return (chosen, jnp.stack([first_member, second], axis=1))
    block_keys = jax.random.split(jax.random.fold_in(base_key, 2), blocks)
    chosen, members = jax.vmap(one_block)(block_keys)
    return (chosen.reshape(TOKENS).astype(jnp.int32), members.reshape(TOKENS, TOP).astype(jnp.int32))


def draw_route_group(key, part):
    return route_table(key)[0]


def draw_route_member(key, part):
    return route_table(key)[1]


def block_scale(key, extent, pieces, smallest, top_value):
    def one(axis_at, shards_of):
        draws = jax.random.uniform(jax.random.fold_in(jax.random.fold_in(key, 6), axis_at), (shards_of,), jnp.float32, smallest / len(pieces), top_value / len(pieces))
        return jnp.repeat(jnp.exp(draws), extent[axis_at] // shards_of).reshape((-1,) + (1,) * (len(extent) - axis_at - 1))

    gain = one(*pieces[0])
    for cut in pieces[1:]:
        gain = gain * one(*cut)
    return gain


def noise(stream_key, extent, scale, most, cuts=(), kind=jnp.bfloat16):
    values = jax.random.normal(stream_key, extent, jnp.float32) * scale
    if len(cuts) > 0:
        values = block_scale(stream_key, extent, cuts, -0.22, 0.18) * values
    return jnp.clip(values, min=-most, max=most).astype(kind)


def setup_inputs(seed: int = 0) -> dict:
    arg_keys = jax.random.split(jax.random.key(seed), 15)
    return {
        "queries": draw_queries(jax.random.fold_in(arg_keys[14], 71), 0),
        "key_heads": draw_key_heads(jax.random.fold_in(arg_keys[14], 71), 0),
        "value_heads": noise(arg_keys[2], (TOKENS, KV_HEADS * HEAD_DIM), 1.0, 4.0, ((0, 16),)),
        "sink_logit": jnp.clip(-2.0 + 9.0 * jax.random.uniform(arg_keys[3], (HEADS,), jnp.float32) ** block_scale(arg_keys[3], (HEADS,), ((0, 16),), -0.2, 0.2), -2.0, 7.0),
        "out_weight": noise(arg_keys[4], (HEADS * HEAD_DIM, D), (HEADS * HEAD_DIM) ** -0.5, 0.125, ((0, 16),)),
        "residual": noise(arg_keys[5], (TOKENS, D), 1.0, 6.0, ((0, 256),)),
        "mixer_gain": jnp.clip(1.0 + 0.18 * jax.random.normal(arg_keys[6], (D,), jnp.float32), 0.1, 1.9),
        "expert_gain": jnp.clip(1.0 + 0.18 * jax.random.normal(arg_keys[7], (D,), jnp.float32), 0.1, 1.9),
        "route_group": draw_route_group(jax.random.fold_in(arg_keys[14], 71), 0),
        "route_member": draw_route_member(jax.random.fold_in(arg_keys[14], 71), 0),
        "route_weight": jnp.clip(0.19921875 + 0.80078125 * jax.random.uniform(arg_keys[10], (TOKENS, TOP), jnp.float32) ** block_scale(arg_keys[10], (TOKENS, TOP), ((0, 256),), -0.2, 0.2), 0.19921875, 1.0).astype(jnp.bfloat16),
        "gate_weight": noise(arg_keys[11], (EXPERTS, D, EXP_HID), D ** -0.5, 0.125, ((0, 16), (2, 16))),
        "up_weight": noise(arg_keys[12], (EXPERTS, D, EXP_HID), D ** -0.5, 0.125, ((0, 16), (2, 16))),
        "down_weight": noise(arg_keys[13], (EXPERTS, EXP_HID, D), EXP_HID ** -0.5, 0.125, ((0, 16), (1, 16))),
    }


EPS = 1e-06
NEG_BIG = -1e+30

def head_attention(queries, key_heads, value_heads, sink_logit):
    blocks = TOKENS // BLOCK
    span_rows = BLOCK + 2 * WINDOW
    key_group = HEADS // KV_HEADS
    query_pos = jnp.arange(TOKENS, dtype=jnp.int32).reshape(blocks, BLOCK)
    key_pos = (jnp.arange(blocks, dtype=jnp.int32) * BLOCK)[:, None] + jnp.arange(span_rows, dtype=jnp.int32)[None, :] - WINDOW
    inside = (jnp.abs(query_pos[:, :, None] - key_pos[:, None, :]) <= WINDOW) & (key_pos >= 0)[:, None, :] & (key_pos < TOKENS)[:, None, :]
    gather_at = jnp.clip(key_pos, 0, TOKENS - 1)

    def one_head(head_index):
        query_cols = lax.dynamic_slice_in_dim(queries, head_index * HEAD_DIM, HEAD_DIM, 1).reshape(blocks, BLOCK, HEAD_DIM)
        kv_start = head_index // key_group * HEAD_DIM
        key_cols = lax.dynamic_slice_in_dim(key_heads, kv_start, HEAD_DIM, 1)[gather_at]
        value_cols = lax.dynamic_slice_in_dim(value_heads, kv_start, HEAD_DIM, 1)[gather_at]
        scores = jnp.einsum('nqd,nkd->nqk', query_cols.astype(jnp.float32), key_cols.astype(jnp.float32)) * HEAD_DIM ** (-0.5)
        scores = jnp.where(inside, scores, NEG_BIG)
        sink_value = sink_logit[head_index].astype(jnp.float32)
        row_top = jnp.maximum(lax.optimization_barrier(jnp.max(scores, axis=2, keepdims=True)), sink_value)
        exp_terms = jnp.exp(scores - row_top)
        row_mass = lax.optimization_barrier(jnp.sum(exp_terms, axis=2, keepdims=True)) + jnp.exp(sink_value - row_top)
        weight = (exp_terms / row_mass).astype(jnp.bfloat16)
        result = jnp.einsum('nqk,nkd->nqd', weight.astype(jnp.float32), value_cols.astype(jnp.float32)).astype(jnp.bfloat16)
        return result.reshape(TOKENS, HEAD_DIM)
    per_head = lax.map(one_head, jnp.arange(HEADS, dtype=jnp.int32))
    return jnp.transpose(per_head, (1, 0, 2)).reshape(TOKENS, HEADS * HEAD_DIM)

def merge_heads(attended, out_weight):
    width = HEADS // N_TP * HEAD_DIM

    def add_block(block_index, running):
        columns = lax.dynamic_slice_in_dim(attended, block_index * width, width, 1)
        weight_rows = lax.dynamic_slice_in_dim(out_weight, block_index * width, width, 0)
        product = jnp.dot(columns, weight_rows, preferred_element_type=jnp.float32).astype(jnp.bfloat16)
        product = lax.optimization_barrier(product)
        return running + product.astype(jnp.float32)
    return lax.fori_loop(0, N_TP, add_block, jnp.zeros((TOKENS, D), jnp.float32))

def reference(queries, key_heads, value_heads, sink_logit, out_weight, residual, mixer_gain, expert_gain, route_group, route_member, route_weight, gate_weight, up_weight, down_weight):
    attended = head_attention(queries, key_heads, value_heads, sink_logit)
    projected = merge_heads(attended, out_weight)
    proj_scale = lax.rsqrt(lax.optimization_barrier(jnp.mean(projected * projected, axis=1, keepdims=True)) + EPS)
    mixed_rows = (residual.astype(jnp.float32) + mixer_gain.astype(jnp.float32) * (projected * proj_scale)).astype(jnp.bfloat16)
    mixed_float = mixed_rows.astype(jnp.float32)
    norm_scale = lax.rsqrt(lax.optimization_barrier(jnp.mean(mixed_float * mixed_float, axis=1, keepdims=True)) + EPS)
    normed = (mixed_float * norm_scale * expert_gain.astype(jnp.float32)).astype(jnp.bfloat16)
    blocks = TOKENS // TOK_DEV
    slots = blocks * GROUP_CAP
    grouped = route_group.reshape(blocks, TOK_DEV)
    chosen = (grouped[:, :, None] == jnp.arange(GROUPS, dtype=jnp.int32)[None, None, :]).astype(jnp.int32)
    group_rank = lax.optimization_barrier(jnp.sum(chosen * (jnp.cumsum(chosen, axis=1) - 1), axis=2))
    block_ids = jnp.arange(blocks, dtype=jnp.int32)[:, None]
    dest = (grouped * slots + block_ids * GROUP_CAP + group_rank).reshape(TOKENS).astype(jnp.int32)
    member_ids = jnp.arange(GROUP_EXPERTS, dtype=jnp.int32)
    token_gates = lax.optimization_barrier(jnp.sum(route_weight.astype(jnp.float32)[:, :, None] * (route_member[:, :, None] == member_ids[None, None, :]).astype(jnp.float32), axis=1))
    slot_rows = jnp.zeros((GROUPS * slots, D), jnp.bfloat16).at[dest].set(normed)
    slot_gates = jnp.zeros((GROUPS * slots, GROUP_EXPERTS), jnp.float32).at[dest].set(token_gates)
    hid_dev = EXP_HID // N_TP

    def group_experts(operands):
        rows_in, gates_in, gate_w, up_w, down_w = operands
        gate_pre = jnp.einsum('md,edh->meh', rows_in.astype(jnp.float32), gate_w.astype(jnp.float32))
        up_pre = jnp.einsum('md,edh->meh', rows_in.astype(jnp.float32), up_w.astype(jnp.float32))
        hidden = (jax.nn.silu(gate_pre) * up_pre * gates_in[:, :, None]).astype(jnp.bfloat16)
        hidden = hidden.reshape(slots, GROUP_EXPERTS, N_TP, hid_dev)
        down_blocks = down_w.reshape(GROUP_EXPERTS, N_TP, hid_dev, D)
        parts = jnp.einsum('mejh,ejhd->mjd', hidden.astype(jnp.float32), down_blocks.astype(jnp.float32))
        parts = lax.optimization_barrier(parts.astype(jnp.bfloat16))
        return lax.optimization_barrier(jnp.sum(parts.astype(jnp.float32), axis=1)).astype(jnp.bfloat16)
    group_out = lax.map(group_experts, (slot_rows.reshape(GROUPS, slots, D), slot_gates.reshape(GROUPS, slots, GROUP_EXPERTS), gate_weight.reshape(GROUPS, GROUP_EXPERTS, D, EXP_HID), up_weight.reshape(GROUPS, GROUP_EXPERTS, D, EXP_HID), down_weight.reshape(GROUPS, GROUP_EXPERTS, EXP_HID, D)))
    expert_out = group_out.reshape(GROUPS * slots, D)[dest]
    return (mixed_float + expert_out.astype(jnp.float32)).astype(jnp.bfloat16)
```

```python
import jax
import jax.numpy as jnp
from jax import lax
from jax.sharding import Mesh
from jax.sharding import PartitionSpec as P

HEADS = 16
KV_HEADS = 4
HEAD_DIM = 128
WINDOW = 128
BLOCK = 128
GROUP_EXPERTS = 3
GROUP_CAP = 10
LANES = 128
Z = "tp_0"
CORE = "tp_1"
TP = (Z, CORE)
SP_TP = ("sp", Z, CORE)
SWAP = [(0, 1), (1, 0)]

EPS = 1e-06
NEG_BIG = -1e30


def extended(block, width):
    count = lax.axis_size("sp")
    forward = [(i, i + 1) for i in range(count - 1)]
    backward = [(target, source) for source, target in forward]
    low = lax.ppermute(block[:, block.shape[1] - width :], "sp", forward)
    high = lax.ppermute(block[:, :width], "sp", backward)
    return jnp.concatenate([low, block, high], axis=1)


def window_attention(queries, key_heads, value_heads, sink_logit):
    seq_rows = queries.shape[0]
    heads_dev = sink_logit.shape[0]
    key_group = HEADS // KV_HEADS
    key_start = lax.axis_index(TP) * heads_dev // key_group * HEAD_DIM
    key_own = lax.dynamic_slice_in_dim(key_heads, key_start, HEAD_DIM, 1)
    value_own = lax.dynamic_slice_in_dim(value_heads, key_start, HEAD_DIM, 1)
    padded = extended(jnp.stack([key_own, value_own]), WINDOW)
    blocks = seq_rows // BLOCK
    extent = WINDOW // BLOCK
    tile_rows = padded.reshape(2, blocks + 2 * extent, BLOCK, HEAD_DIM)
    key_spans = jnp.concatenate(
        [tile_rows[:, shifted : shifted + blocks] for shifted in range(2 * extent + 1)], axis=2
    )
    offset = lax.axis_index("sp") * seq_rows
    seq_total = seq_rows * lax.axis_size("sp")
    query_pos = offset + jnp.arange(seq_rows, dtype=jnp.int32).reshape(blocks, BLOCK)
    key_pos = (
        offset
        + (jnp.arange(blocks, dtype=jnp.int32) * BLOCK)[:, None]
        + jnp.arange(BLOCK + 2 * WINDOW, dtype=jnp.int32)[None, :]
        - WINDOW
    )
    inside = (
        (jnp.abs(query_pos[:, :, None] - key_pos[:, None, :]) <= WINDOW)
        & (key_pos >= 0)[:, None, :]
        & (key_pos < seq_total)[:, None, :]
    )
    query_blocks = queries.reshape(blocks, BLOCK, heads_dev, HEAD_DIM)
    scores = jnp.einsum(
        "nqhd,nkd->nhqk", query_blocks, key_spans[0], preferred_element_type=jnp.float32
    ) * HEAD_DIM ** (-0.5)
    scores = jnp.where(inside[:, None], scores, NEG_BIG)
    sink_col = sink_logit[None, :, None, None]
    row_top = jnp.maximum(jnp.max(scores, axis=3, keepdims=True), sink_col)
    exp_terms = jnp.exp(scores - row_top)
    row_mass = jnp.sum(exp_terms, axis=3, keepdims=True) + jnp.exp(sink_col - row_top)
    weight = (exp_terms / row_mass).astype(jnp.bfloat16)
    attended = jnp.einsum(
        "nhqk,nkd->nqhd", weight, key_spans[1], preferred_element_type=jnp.float32
    ).astype(jnp.bfloat16)
    return attended.reshape(seq_rows, heads_dev * HEAD_DIM)


def per_device(
    queries,
    key_heads,
    value_heads,
    sink_logit,
    out_weight,
    residual,
    mixer_gain,
    expert_gain,
    route_group,
    route_member,
    route_weight,
    gate_weight,
    up_weight,
    down_weight,
):
    depth = lax.axis_size(Z)
    groups = lax.axis_size("sp")
    core = lax.axis_index(CORE)
    tok_rows, width = residual.shape
    capacity = GROUP_CAP
    slots = groups * capacity

    weight_rows = lax.all_gather(out_weight, Z, axis=0, tiled=False)
    attended = window_attention(queries, key_heads, value_heads, sink_logit)
    by_chip = lax.all_to_all(
        attended.reshape(depth, 2, tok_rows, HEAD_DIM), Z, split_axis=0, concat_axis=0, tiled=True
    )

    def head_sum(which):
        rows = lax.dynamic_index_in_dim(by_chip, which, 1, False)
        return jnp.einsum("zrk,zkn->rn", rows, weight_rows, preferred_element_type=jnp.float32)

    from_partner = lax.ppermute(head_sum(1 - core).astype(jnp.bfloat16), CORE, SWAP)
    projected = head_sum(core) + from_partner.astype(jnp.float32)
    proj_scale = lax.rsqrt(jnp.mean(projected * projected, axis=1, keepdims=True) + EPS)
    mixed_rows = (residual.astype(jnp.float32) + mixer_gain * (projected * proj_scale)).astype(
        jnp.bfloat16
    )
    mixed_float = mixed_rows.astype(jnp.float32)
    norm_scale = lax.rsqrt(jnp.mean(mixed_float * mixed_float, axis=1, keepdims=True) + EPS)
    normed = (mixed_float * norm_scale * expert_gain).astype(jnp.bfloat16)

    group_ids = jnp.arange(groups, dtype=jnp.int32)
    chosen = (route_group[:, None] == group_ids[None, :]).astype(jnp.int32)
    group_rank = jnp.sum(chosen * (jnp.cumsum(chosen, axis=0) - 1), axis=1)
    slot_ids = route_group * capacity + group_rank
    placing = (jnp.arange(slots, dtype=jnp.int32)[:, None] == slot_ids[None, :]).astype(
        jnp.bfloat16
    )
    member_ids = jnp.arange(GROUP_EXPERTS, dtype=jnp.int32)
    token_gates = jnp.sum(
        route_weight.astype(jnp.float32)[:, :, None]
        * (route_member[:, :, None] == member_ids[None, None, :]).astype(jnp.float32),
        axis=1,
    ).astype(jnp.bfloat16)
    send_gates = jnp.dot(placing, token_gates, preferred_element_type=jnp.float32).astype(
        jnp.bfloat16
    )
    send_gates = send_gates.reshape(groups, capacity * GROUP_EXPERTS)
    send_gates = jnp.pad(send_gates, ((0, 0), (0, LANES - capacity * GROUP_EXPERTS)))
    arrived_gates = lax.all_to_all(send_gates, "sp", split_axis=0, concat_axis=0, tiled=True)
    pooled_gates = lax.all_gather(arrived_gates, Z, axis=0, tiled=True)
    flat_gates = (
        pooled_gates[:, : capacity * GROUP_EXPERTS]
        .reshape(depth * slots, GROUP_EXPERTS)
        .astype(jnp.float32)
    )

    def chip_weights(shard, dim):
        return jnp.concatenate([shard, lax.ppermute(shard, CORE, SWAP)], axis=dim)

    gate_chip = chip_weights(gate_weight, 2)
    up_chip = chip_weights(up_weight, 2)
    down_chip = chip_weights(down_weight, 1)
    hid = gate_chip.shape[2]

    send_rows = jnp.dot(placing, normed, preferred_element_type=jnp.float32).astype(jnp.bfloat16)
    arrived = lax.all_to_all(
        send_rows.reshape(groups, capacity * width // LANES, LANES),
        "sp",
        split_axis=0,
        concat_axis=0,
        tiled=True,
    )
    flat_rows = lax.all_gather(arrived.reshape(slots, width), Z, axis=0, tiled=True)
    hidden = []
    for e in range(GROUP_EXPERTS):
        gate_pre = jnp.dot(flat_rows, gate_chip[e], preferred_element_type=jnp.float32)
        up_pre = jnp.dot(flat_rows, up_chip[e], preferred_element_type=jnp.float32)
        gated = jax.nn.silu(gate_pre) * up_pre * flat_gates[:, e : e + 1]
        hidden.append(gated.astype(jnp.bfloat16))
    partial_out = jnp.dot(
        jnp.concatenate(hidden, axis=1),
        down_chip.reshape(GROUP_EXPERTS * hid, width),
        preferred_element_type=jnp.float32,
    ).astype(jnp.bfloat16)
    summed = lax.psum_scatter(partial_out, Z, scatter_dimension=0, tiled=True)
    returned = lax.all_to_all(
        summed.reshape(groups, capacity * width // LANES, LANES),
        "sp",
        split_axis=0,
        concat_axis=0,
        tiled=True,
    )
    expert_out = lax.dot_general(
        placing,
        returned.reshape(slots, width),
        (((0,), (0,)), ((), ())),
        preferred_element_type=jnp.float32,
    )
    return (mixed_float + expert_out).astype(jnp.bfloat16)


def solution(mesh):
    torus = Mesh(mesh.devices.reshape(mesh.shape["sp"], 8, 2), ("sp", Z, CORE))
    placed = (
        P("sp", TP),
        P("sp", None),
        P("sp", None),
        P(TP),
        P(TP, None),
        P(SP_TP, None),
        P(),
        P(),
        P(SP_TP),
        P(SP_TP, None),
        P(SP_TP, None),
        P("sp", None, TP),
        P("sp", None, TP),
        P("sp", TP, None),
    )
    return jax.shard_map(
        per_device, mesh=torus, in_specs=placed, out_specs=P(SP_TP, None), check_vma=False
    )
```

```python
import jax
import jax.numpy as jnp
from jax import lax
from jax.experimental import pallas as pl
from jax.experimental.pallas import tpu as pltpu
from jax.sharding import Mesh
from jax.sharding import PartitionSpec as P

HEADS = 16
KV_HEADS = 4
HEAD_DIM = 128
WINDOW = 128
BLOCK = 128
GROUP_EXPERTS = 3
GROUP_CAP = 10
LANES = 128
Z = "tp_0"
CORE = "tp_1"
TP = (Z, CORE)
SP_TP = ("sp", Z, CORE)
SWAP = [(0, 1), (1, 0)]

EPS = 1e-06
NEG_BIG = -1e30


def extended(block, width):
    count = lax.axis_size("sp")
    forward = [(i, i + 1) for i in range(count - 1)]
    backward = [(target, source) for source, target in forward]
    low = lax.ppermute(block[:, block.shape[1] - width :], "sp", forward)
    high = lax.ppermute(block[:, :width], "sp", backward)
    return jnp.concatenate([low, block, high], axis=1)


def chip_attention(queries, key_heads, value_heads, sink_logit):
    seq_rows = queries.shape[0]
    core = lax.axis_index(CORE)
    key_start = lax.axis_index(Z) * 2 * KV_HEADS // HEADS * HEAD_DIM
    key_own = lax.dynamic_slice_in_dim(key_heads, key_start, HEAD_DIM, 1)
    value_own = lax.dynamic_slice_in_dim(value_heads, key_start, HEAD_DIM, 1)
    padded = extended(jnp.stack([key_own, value_own]), WINDOW)
    blocks = seq_rows // (2 * BLOCK)
    query_blocks = queries.reshape(blocks, 2, BLOCK, HEAD_DIM)
    query_far = lax.ppermute(
        lax.dynamic_index_in_dim(query_blocks, 1 - core, 1, True), CORE, SWAP
    )
    query_pair = jnp.concatenate(
        [lax.dynamic_index_in_dim(query_blocks, core, 1, True), query_far], axis=1
    )
    sink_pair = jnp.concatenate([sink_logit, lax.ppermute(sink_logit, CORE, SWAP)])
    tile_rows = padded.reshape(2, 2 * blocks + 2, BLOCK, HEAD_DIM)
    key_spans = jnp.concatenate(
        [
            lax.dynamic_slice_in_dim(tile_rows, core + shifted, 2 * blocks - 1, 1)[:, ::2]
            for shifted in range(3)
        ],
        axis=2,
    )
    offset = lax.axis_index("sp") * seq_rows
    seq_total = seq_rows * lax.axis_size("sp")
    block_start = offset + (2 * jnp.arange(blocks, dtype=jnp.int32) + core) * BLOCK
    query_pos = block_start[:, None] + jnp.arange(BLOCK, dtype=jnp.int32)[None, :]
    key_pos = (
        block_start[:, None] + jnp.arange(BLOCK + 2 * WINDOW, dtype=jnp.int32)[None, :] - WINDOW
    )
    inside = (
        (jnp.abs(query_pos[:, :, None] - key_pos[:, None, :]) <= WINDOW)
        & (key_pos >= 0)[:, None, :]
        & (key_pos < seq_total)[:, None, :]
    )
    scores = jnp.einsum(
        "nhqd,nkd->nhqk", query_pair, key_spans[0], preferred_element_type=jnp.float32
    ) * HEAD_DIM ** (-0.5)
    scores = jnp.where(inside[:, None], scores, NEG_BIG)
    sink_col = sink_pair[None, :, None, None]
    row_top = jnp.maximum(jnp.max(scores, axis=3, keepdims=True), sink_col)
    exp_terms = jnp.exp(scores - row_top)
    row_mass = jnp.sum(exp_terms, axis=3, keepdims=True) + jnp.exp(sink_col - row_top)
    weight = (exp_terms / row_mass).astype(jnp.bfloat16)
    return jnp.einsum(
        "nhqk,nkd->nhqd", weight, key_spans[1], preferred_element_type=jnp.float32
    ).astype(jnp.bfloat16)


MAIN_CAP = 7
REL = (0, -1, 1, -2, 2, -3, 3, 4)


def shifts():
    n = lax.axis_size(Z)
    up = [(i, (i + 1) % n) for i in range(n)]
    down = [(i, (i - 1) % n) for i in range(n)]
    return (lambda a: lax.ppermute(a, Z, up)), (lambda a: lax.ppermute(a, Z, down))


def ring_gather(block):
    up, down = shifts()
    half = block.shape[1] // 2
    blocks, low, high = [block], block, block
    for _ in range(3):
        low, high = up(low), down(high)
        blocks += [low, high]
    far = jnp.concatenate([up(low[:, :half]), down(high[:, half:])], axis=1)
    return blocks + [far]


def ring_reduce(parts):
    up, down = shifts()
    half = parts[0].shape[1] // 2
    low, high = up(parts[4][:, :half]), down(parts[4][:, half:])
    low = jnp.concatenate([parts[3][:, :half] + low, parts[3][:, half:]], axis=1)
    high = jnp.concatenate([parts[-3][:, :half], parts[-3][:, half:] + high], axis=1)
    for step in (2, 1):
        low, high = parts[step] + up(low), parts[-step] + down(high)
    return parts[0] + up(low) + down(high)


def in_ring_order(blocks, near_first):
    me = lax.axis_index(Z)
    n = lax.axis_size(Z)
    return [lax.dynamic_index_in_dim(blocks, (me + r) % n, 0, False) for r in near_first]


def experts_kernel(
    rows, gates, gate_own, gate_far, up_own, up_far, down_own, down_far, out, hidden
):
    e = pl.program_id(0)
    total, width = rows.shape
    step = total // (1 + total // 512)
    hid = 2 * gate_own.shape[2]
    wide = 512

    @pl.loop(0, total // step)
    def _(i):
        at = pl.ds(pl.multiple_of(i * step, 16), step)

        for k in range(GROUP_EXPERTS):

            @pl.when(e == k)
            def _():
                weights = jnp.concatenate(
                    [gate_own[0], gate_far[0], up_own[0], up_far[0]], axis=1
                )
                both = jnp.dot(rows[at, :], weights, preferred_element_type=jnp.float32)
                pre = both[:, :hid]
                gated = pre / (1.0 + jnp.exp(-pre)) * both[:, hid:] * gates[0, at, :]
                hidden[at, k * hid : (k + 1) * hid] = gated.astype(jnp.bfloat16)

        @pl.when(e == GROUP_EXPERTS)
        def _():
            pieces = []
            for k in range(GROUP_EXPERTS):
                pieces += [down_own[k], down_far[k]]
            for c in range(0, width, wide):
                cols = slice(c, c + wide)
                down = jnp.concatenate([p[:, cols] for p in pieces], axis=0)
                out[at, cols] = jnp.dot(
                    hidden[at, :], down, preferred_element_type=jnp.float32
                ).astype(jnp.bfloat16)


def experts(rows, gates, gate_pair, up_pair, down_pair):
    total, width = rows.shape
    hid = gate_pair[0].shape[2]
    last = GROUP_EXPERTS - 1
    into = pl.BlockSpec((1, width, hid), lambda e: (jnp.minimum(e, last), 0, 0))
    outof = pl.BlockSpec(
        (GROUP_EXPERTS, hid, width), lambda e: (0, 0, 0), pipeline_mode=pl.Buffered(1)
    )
    whole = pl.BlockSpec((total, width), lambda e: (0, 0), pipeline_mode=pl.Buffered(1))
    work = total * width * hid * 2 * GROUP_EXPERTS
    return pl.pallas_call(
        experts_kernel,
        grid=(GROUP_EXPERTS + 1,),
        in_specs=[
            whole,
            pl.BlockSpec((1, total, 1), lambda e: (jnp.minimum(e, last), 0, 0)),
            into,
            into,
            into,
            into,
            outof,
            outof,
        ],
        out_specs=pl.BlockSpec((total, width), lambda e: (0, 0)),
        out_shape=jax.ShapeDtypeStruct((total, width), jnp.bfloat16),
        scratch_shapes=[pltpu.VMEM((total, GROUP_EXPERTS * 2 * hid), jnp.bfloat16)],
        compiler_params=pltpu.CompilerParams(
            dimension_semantics=("arbitrary",), vmem_limit_bytes=48 * 2**20
        ),
        cost_estimate=pl.CostEstimate(
            flops=6 * work, bytes_accessed=20 * 2**20, transcendentals=total * hid * 6
        ),
        name="experts",
    )(rows, gates.T[:, :, None], *gate_pair, *up_pair, *down_pair)


def per_device(
    queries,
    key_heads,
    value_heads,
    sink_logit,
    out_weight,
    residual,
    mixer_gain,
    expert_gain,
    route_group,
    route_member,
    route_weight,
    gate_weight,
    up_weight,
    down_weight,
):
    depth = lax.axis_size(Z)
    groups = lax.axis_size("sp")
    width = residual.shape[1]
    capacity = GROUP_CAP
    slots = groups * capacity
    cap_a = MAIN_CAP
    cap_b = capacity - cap_a
    slots_a, slots_b = groups * cap_a, groups * cap_b


    gate_pair, up_pair, down_pair = (
        (shard, lax.ppermute(shard, CORE, SWAP))
        for shard in (gate_weight, up_weight, down_weight)
    )

    group_ids = jnp.arange(groups, dtype=jnp.int32)
    chosen = (route_group[:, None] == group_ids[None, :]).astype(jnp.int32)
    group_rank = jnp.sum(chosen * (jnp.cumsum(chosen, axis=0) - 1), axis=1)
    slot_ids = route_group * capacity + group_rank
    placing = (jnp.arange(slots, dtype=jnp.int32)[:, None] == slot_ids[None, :]).astype(
        jnp.bfloat16
    )
    member_ids = jnp.arange(GROUP_EXPERTS, dtype=jnp.int32)
    token_gates = jnp.sum(
        route_weight.astype(jnp.float32)[:, :, None]
        * (route_member[:, :, None] == member_ids[None, None, :]).astype(jnp.float32),
        axis=1,
    ).astype(jnp.bfloat16)
    send_gates = jnp.dot(placing, token_gates, preferred_element_type=jnp.float32).astype(
        jnp.bfloat16
    )
    gate_cols = capacity * GROUP_EXPERTS
    send_gates = jnp.pad(
        send_gates.reshape(groups, gate_cols), ((0, 0), (0, LANES - gate_cols))
    )

    weight_pair = jnp.stack([out_weight, lax.ppermute(out_weight, CORE, SWAP)])
    attended = chip_attention(queries, key_heads, value_heads, sink_logit)
    head_part = jnp.einsum(
        "nhqd,hdm->nqm", attended, weight_pair, preferred_element_type=jnp.float32
    ).astype(jnp.bfloat16)
    projected = lax.psum_scatter(
        head_part.reshape(-1, width), Z, scatter_dimension=0, tiled=True
    ).astype(jnp.float32)

    send_gates, head_part = lax.optimization_barrier((send_gates, head_part))
    arrived_gates = lax.all_to_all(send_gates, "sp", split_axis=0, concat_axis=0, tiled=True)
    pooled_gates = lax.all_to_all(
        jnp.broadcast_to(arrived_gates[None], (depth, groups, LANES)),
        Z,
        split_axis=0,
        concat_axis=0,
        tiled=True,
    )
    pooled_gates = pooled_gates[:, :, :gate_cols].astype(jnp.float32)
    pooled_gates = pooled_gates.reshape(depth, groups, capacity, GROUP_EXPERTS)
    gates_a = pooled_gates[:, :, :cap_a].reshape(depth * slots_a, GROUP_EXPERTS)
    gates_b = pooled_gates[:, :, cap_a:].reshape(depth, slots_b, GROUP_EXPERTS)
    gates_b = jnp.concatenate(in_ring_order(gates_b, REL), axis=0)
    projected, gate_pair, up_pair, down_pair, gates_a, gates_b = lax.optimization_barrier(
        (projected, gate_pair, up_pair, down_pair, gates_a, gates_b)
    )

    proj_scale = lax.rsqrt(jnp.mean(projected * projected, axis=1, keepdims=True) + EPS)
    mixed_rows = (residual.astype(jnp.float32) + mixer_gain * (projected * proj_scale)).astype(
        jnp.bfloat16
    )
    mixed_float = mixed_rows.astype(jnp.float32)
    norm_scale = lax.rsqrt(jnp.mean(mixed_float * mixed_float, axis=1, keepdims=True) + EPS)
    normed = (mixed_float * norm_scale * expert_gain).astype(jnp.bfloat16)

    def exchange(rows):
        return lax.all_to_all(
            rows.reshape(groups, -1, LANES), "sp", split_axis=0, concat_axis=0, tiled=True
        )

    send_rows = jnp.dot(placing, normed, preferred_element_type=jnp.float32).astype(jnp.bfloat16)
    arrived = exchange(send_rows)
    cut = cap_a * width // LANES
    pool_a = lax.all_gather(arrived[:, :cut].reshape(slots_a, width), Z, axis=0, tiled=True)
    pool_b = ring_gather(arrived[:, cut:].reshape(slots_b, width))

    part_b = experts(jnp.concatenate(pool_b, axis=0), gates_b, gate_pair, up_pair, down_pair)
    pool_a, part_b = lax.optimization_barrier((pool_a, part_b))
    part_a = experts(pool_a, gates_a, gate_pair, up_pair, down_pair)
    sum_a = lax.psum_scatter(part_a, Z, scatter_dimension=0, tiled=True)
    sum_b = ring_reduce(
        {r: part_b[k * slots_b : (k + 1) * slots_b] for k, r in enumerate(REL)}
    )
    back_b = exchange(sum_b)
    back_a = exchange(sum_a)
    returned = jnp.concatenate([back_a, back_b], axis=1).reshape(slots, width)
    expert_out = lax.dot_general(
        placing,
        returned,
        (((0,), (0,)), ((), ())),
        preferred_element_type=jnp.float32,
    )
    return (mixed_float + expert_out).astype(jnp.bfloat16)


def solution(mesh):
    torus = Mesh(mesh.devices.reshape(mesh.shape["sp"], 8, 2), ("sp", Z, CORE))
    placed = (
        P("sp", TP),
        P("sp", None),
        P("sp", None),
        P(TP),
        P(TP, None),
        P(SP_TP, None),
        P(),
        P(),
        P(SP_TP),
        P(SP_TP, None),
        P(SP_TP, None),
        P("sp", None, TP),
        P("sp", None, TP),
        P("sp", TP, None),
    )
    return jax.shard_map(
        per_device, mesh=torus, in_specs=placed, out_specs=P(SP_TP, None), check_vma=False
    )
```

```python
import jax
import jax.numpy as jnp
from jax import lax
from jax.experimental import pallas as pl
from jax.experimental.pallas import tpu as pltpu
from jax.sharding import Mesh
from jax.sharding import PartitionSpec as P


HEADS = 16
KV_HEADS = 4
HEAD_DIM = 128
WINDOW = 128
BLOCK = 128
GROUP_EXPERTS = 3
GROUP_CAP = 10
LANES = 128
Z = "tp_0"
CORE = "tp_1"
TP = (Z, CORE)
SP_TP = ("sp", Z, CORE)
SWAP = [(0, 1), (1, 0)]

EPS = 1e-06
NEG_BIG = -1e30


def extended(block, width):
    count = lax.axis_size("sp")
    forward = [(i, i + 1) for i in range(count - 1)]
    backward = [(target, source) for source, target in forward]
    low = lax.ppermute(block[:, block.shape[1] - width :], "sp", forward)
    high = lax.ppermute(block[:, :width], "sp", backward)
    return jnp.concatenate([low, block, high], axis=1)


def chip_attention(queries, key_heads, value_heads, sink_logit):
    seq_rows = queries.shape[0]
    core = lax.axis_index(CORE)
    key_start = lax.axis_index(Z) * 2 * KV_HEADS // HEADS * HEAD_DIM
    key_own = lax.dynamic_slice_in_dim(key_heads, key_start, HEAD_DIM, 1)
    value_own = lax.dynamic_slice_in_dim(value_heads, key_start, HEAD_DIM, 1)
    padded = extended(jnp.stack([key_own, value_own]), WINDOW)
    blocks = seq_rows // (2 * BLOCK)
    query_blocks = queries.reshape(blocks, 2, BLOCK, HEAD_DIM)
    query_far = lax.ppermute(
        lax.dynamic_index_in_dim(query_blocks, 1 - core, 1, True), CORE, SWAP
    )
    query_pair = jnp.concatenate(
        [lax.dynamic_index_in_dim(query_blocks, core, 1, True), query_far], axis=1
    )
    sink_pair = jnp.concatenate([sink_logit, lax.ppermute(sink_logit, CORE, SWAP)])
    tile_rows = padded.reshape(2, 2 * blocks + 2, BLOCK, HEAD_DIM)
    key_spans = jnp.concatenate(
        [
            lax.dynamic_slice_in_dim(tile_rows, core + shifted, 2 * blocks - 1, 1)[:, ::2]
            for shifted in range(3)
        ],
        axis=2,
    )
    offset = lax.axis_index("sp") * seq_rows
    seq_total = seq_rows * lax.axis_size("sp")
    block_start = offset + (2 * jnp.arange(blocks, dtype=jnp.int32) + core) * BLOCK
    query_pos = block_start[:, None] + jnp.arange(BLOCK, dtype=jnp.int32)[None, :]
    key_pos = (
        block_start[:, None] + jnp.arange(BLOCK + 2 * WINDOW, dtype=jnp.int32)[None, :] - WINDOW
    )
    inside = (
        (jnp.abs(query_pos[:, :, None] - key_pos[:, None, :]) <= WINDOW)
        & (key_pos >= 0)[:, None, :]
        & (key_pos < seq_total)[:, None, :]
    )
    scores = jnp.einsum(
        "nhqd,nkd->nhqk", query_pair, key_spans[0], preferred_element_type=jnp.float32
    ) * HEAD_DIM ** (-0.5)
    scores = jnp.where(inside[:, None], scores, NEG_BIG)
    sink_col = sink_pair[None, :, None, None]
    row_top = jnp.maximum(jnp.max(scores, axis=3, keepdims=True), sink_col)
    exp_terms = jnp.exp(scores - row_top)
    row_mass = jnp.sum(exp_terms, axis=3, keepdims=True) + jnp.exp(sink_col - row_top)
    weight = (exp_terms / row_mass).astype(jnp.bfloat16)
    return jnp.einsum(
        "nhqk,nkd->nhqd", weight, key_spans[1], preferred_element_type=jnp.float32
    ).astype(jnp.bfloat16)


MAIN_CAP = 7
MAIN_COLS = 1280
REL = (0, -1, 1, -2, 2, -3, 3, 4)


def shifts():
    n = lax.axis_size(Z)
    up = [(i, (i + 1) % n) for i in range(n)]
    down = [(i, (i - 1) % n) for i in range(n)]
    return (lambda a: lax.ppermute(a, Z, up)), (lambda a: lax.ppermute(a, Z, down))


def ring_gather(block):
    up, down = shifts()
    half = block.shape[1] // (2 * LANES) * LANES
    blocks, low, high = [block], block, block
    for _ in range(3):
        low, high = up(low), down(high)
        blocks += [low, high]
    far = jnp.concatenate([up(low[:, :half]), down(high[:, half:])], axis=1)
    return blocks + [far]


def ring_reduce(parts):
    up, down = shifts()
    half = parts[0].shape[1] // 2
    low, high = up(parts[4][:, :half]), down(parts[4][:, half:])
    low = jnp.concatenate([parts[3][:, :half] + low, parts[3][:, half:]], axis=1)
    high = jnp.concatenate([parts[-3][:, :half], parts[-3][:, half:] + high], axis=1)
    for step in (2, 1):
        low, high = parts[step] + up(low), parts[-step] + down(high)
    return parts[0] + up(low) + down(high)


def in_ring_order(blocks, near_first):
    me = lax.axis_index(Z)
    n = lax.axis_size(Z)
    return [lax.dynamic_index_in_dim(blocks, (me + r) % n, 0, False) for r in near_first]


def experts_kernel(rows_in, *refs):
    weights_in, out_to = refs[:6], refs[6]
    weights, (rows, hidden, out) = refs[7:13], refs[13:16]
    weight_sems, row_sems, out_sems = refs[16:]
    gate_own, gate_far, up_own, up_far, down_own, down_far = weights
    total = rows.shape[0]
    width = out.shape[1]
    hid = 2 * gate_own.shape[2]
    steps = 1 + total // 512
    step = total // steps
    spans = [slice(i * step, (i + 1) * step) for i in range(steps)]
    wide = 512

    def weight_copy(k, e):
        return pltpu.make_async_copy(weights_in[k].at[e], weights[k].at[e], weight_sems.at[k, e])

    def row_copy(i):
        return pltpu.make_async_copy(rows_in.at[spans[i]], rows.at[spans[i]], row_sems.at[i])

    def out_copy(i):
        return pltpu.make_async_copy(out.at[spans[i]], out_to.at[spans[i]], out_sems.at[i])

    for k in range(4):
        weight_copy(k, 0).start()
    for i in range(steps):
        row_copy(i).start()
    for e in range(1, GROUP_EXPERTS):
        for k in range(4):
            weight_copy(k, e).start()
    for e in range(GROUP_EXPERTS):
        for k in (4, 5):
            weight_copy(k, e).start()

    for e in range(GROUP_EXPERTS):
        for k in range(4):
            weight_copy(k, e).wait()
        for i in range(steps):
            if e == 0:
                row_copy(i).wait()
            joined = jnp.concatenate([gate_own[e], gate_far[e], up_own[e], up_far[e]], axis=1)
            both = jnp.dot(rows[spans[i], :width], joined, preferred_element_type=jnp.float32)
            pre = both[:, :hid]
            gated = pre / (1.0 + jnp.exp(-pre)) * both[:, hid:]
            gated = gated * rows[spans[i], width + e : width + e + 1].astype(jnp.float32)
            hidden[spans[i], e * hid : (e + 1) * hid] = gated.astype(jnp.bfloat16)
    for e in range(GROUP_EXPERTS):
        for k in (4, 5):
            weight_copy(k, e).wait()
    for i in range(steps):
        for c in range(0, width, wide):
            cols = slice(c, c + wide)
            pieces = []
            for e in range(GROUP_EXPERTS):
                pieces += [down_own[e, :, cols], down_far[e, :, cols]]
            out[spans[i], cols] = jnp.dot(
                hidden[spans[i], :],
                jnp.concatenate(pieces, axis=0),
                preferred_element_type=jnp.float32,
            ).astype(jnp.bfloat16)
        out_copy(i).start()
    for i in range(steps):
        out_copy(i).wait()


def experts(rows, gate_pair, up_pair, down_pair):
    total, lanes = rows.shape
    width = lanes - LANES
    hid = gate_pair[0].shape[2]
    steps = 1 + total // 512
    work = total * width * hid * 2 * GROUP_EXPERTS
    anywhere = pl.BlockSpec(memory_space=pltpu.HBM)
    into = pltpu.VMEM((GROUP_EXPERTS, width, hid), jnp.bfloat16)
    outof = pltpu.VMEM((GROUP_EXPERTS, hid, width), jnp.bfloat16)
    return pl.pallas_call(
        experts_kernel,
        in_specs=[anywhere] * 7,
        out_specs=anywhere,
        out_shape=jax.ShapeDtypeStruct((total, width), jnp.bfloat16),
        scratch_shapes=[into] * 4
        + [outof] * 2
        + [
            pltpu.VMEM((total, lanes), jnp.bfloat16),
            pltpu.VMEM((total, GROUP_EXPERTS * 2 * hid), jnp.bfloat16),
            pltpu.VMEM((total, width), jnp.bfloat16),
            pltpu.SemaphoreType.DMA((6, GROUP_EXPERTS)),
            pltpu.SemaphoreType.DMA((steps,)),
            pltpu.SemaphoreType.DMA((steps,)),
        ],
        compiler_params=pltpu.CompilerParams(vmem_limit_bytes=62 * 2**20),
        cost_estimate=pl.CostEstimate(
            flops=6 * work, bytes_accessed=20 * 2**20, transcendentals=total * hid * 6
        ),
        name="experts",
    )(rows, *gate_pair, *up_pair, *down_pair)


def per_device(
    queries,
    key_heads,
    value_heads,
    sink_logit,
    out_weight,
    residual,
    mixer_gain,
    expert_gain,
    route_group,
    route_member,
    route_weight,
    gate_weight,
    up_weight,
    down_weight,
):
    groups = lax.axis_size("sp")
    width = residual.shape[1]
    capacity = GROUP_CAP
    slots = groups * capacity
    cap_a = MAIN_CAP
    cap_b = capacity - cap_a
    slots_b = groups * cap_b


    gate_pair, up_pair, down_pair = (
        (shard, lax.ppermute(shard, CORE, SWAP))
        for shard in (gate_weight, up_weight, down_weight)
    )

    group_ids = jnp.arange(groups, dtype=jnp.int32)
    chosen = (route_group[:, None] == group_ids[None, :]).astype(jnp.int32)
    group_rank = jnp.sum(chosen * (jnp.cumsum(chosen, axis=0) - 1), axis=1)
    slot_ids = route_group * capacity + group_rank
    placing = (jnp.arange(slots, dtype=jnp.int32)[:, None] == slot_ids[None, :]).astype(
        jnp.bfloat16
    )
    member_ids = jnp.arange(GROUP_EXPERTS, dtype=jnp.int32)
    token_gates = jnp.sum(
        route_weight.astype(jnp.float32)[:, :, None]
        * (route_member[:, :, None] == member_ids[None, None, :]).astype(jnp.float32),
        axis=1,
    ).astype(jnp.bfloat16)
    send_gates = jnp.dot(
        placing,
        jnp.pad(token_gates, ((0, 0), (0, LANES - GROUP_EXPERTS))),
        preferred_element_type=jnp.float32,
    ).astype(jnp.bfloat16)
    send_gates = jnp.pad(
        send_gates.reshape(groups, capacity, LANES), ((0, 0), (0, 16 - capacity), (0, 0))
    )

    weight_pair = jnp.stack([out_weight, lax.ppermute(out_weight, CORE, SWAP)])
    attended = chip_attention(queries, key_heads, value_heads, sink_logit)

    def head_part(cols):
        return jnp.einsum(
            "nhqd,hdm->nqm", attended, weight_pair[:, :, cols], preferred_element_type=jnp.float32
        ).astype(jnp.bfloat16)

    ring_part = head_part(slice(MAIN_COLS, width))
    main_part = head_part(slice(0, MAIN_COLS)).reshape(-1, MAIN_COLS)
    main_sum = lax.psum_scatter(main_part, Z, scatter_dimension=0, tiled=True)
    ring_sum = ring_reduce(dict(zip(REL, in_ring_order(ring_part, REL))))
    projected = jnp.concatenate([main_sum, ring_sum], axis=1).astype(jnp.float32)
    projected, gate_pair, up_pair, down_pair = lax.optimization_barrier(
        (projected, gate_pair, up_pair, down_pair)
    )

    proj_scale = lax.rsqrt(jnp.mean(projected * projected, axis=1, keepdims=True) + EPS)
    mixed_rows = (residual.astype(jnp.float32) + mixer_gain * (projected * proj_scale)).astype(
        jnp.bfloat16
    )
    mixed_float = mixed_rows.astype(jnp.float32)
    norm_scale = lax.rsqrt(jnp.mean(mixed_float * mixed_float, axis=1, keepdims=True) + EPS)
    normed = (mixed_float * norm_scale * expert_gain).astype(jnp.bfloat16)

    def exchange(rows):
        return lax.all_to_all(
            rows.reshape(groups, -1, LANES), "sp", split_axis=0, concat_axis=0, tiled=True
        )

    send_rows = jnp.dot(placing, normed, preferred_element_type=jnp.float32).astype(jnp.bfloat16)
    send_rows = send_rows.reshape(groups, capacity * width // LANES, LANES)
    tiles = width // LANES
    arrived = exchange(jnp.concatenate([send_rows, send_gates], axis=1))

    def with_gates(low, high):
        rows = arrived[:, low * tiles : high * tiles].reshape(-1, width)
        gates = arrived[:, capacity * tiles + low : capacity * tiles + high].reshape(-1, LANES)
        return jnp.concatenate([rows, gates], axis=1)

    pool_a = lax.all_gather(with_gates(0, cap_a), Z, axis=0, tiled=True)
    pool_b = ring_gather(with_gates(cap_a, capacity))
    part_b = experts(jnp.concatenate(pool_b, axis=0), gate_pair, up_pair, down_pair)
    pool_a, part_b = lax.optimization_barrier((pool_a, part_b))
    part_a = experts(pool_a, gate_pair, up_pair, down_pair)
    sum_a = lax.psum_scatter(part_a, Z, scatter_dimension=0, tiled=True)
    sum_b = ring_reduce(
        {r: part_b[k * slots_b : (k + 1) * slots_b] for k, r in enumerate(REL)}
    )
    back_b = exchange(sum_b)
    back_a = exchange(sum_a)
    returned = jnp.concatenate([back_a, back_b], axis=1).reshape(slots, width)
    expert_out = lax.dot_general(
        placing,
        returned,
        (((0,), (0,)), ((), ())),
        preferred_element_type=jnp.float32,
    )
    return (mixed_float + expert_out).astype(jnp.bfloat16)


def solution(mesh):
    torus = Mesh(mesh.devices.reshape(mesh.shape["sp"], 8, 2), ("sp", Z, CORE))
    placed = (
        P("sp", TP),
        P("sp", None),
        P("sp", None),
        P(TP),
        P(TP, None),
        P(SP_TP, None),
        P(),
        P(),
        P(SP_TP),
        P(SP_TP, None),
        P(SP_TP, None),
        P("sp", None, TP),
        P("sp", None, TP),
        P("sp", TP, None),
    )

    return jax.shard_map(
        per_device, mesh=torus, in_specs=placed, out_specs=P(SP_TP, None), check_vma=False
    )
```

```python
import jax
import jax.numpy as jnp
from jax import lax
from jax.experimental import pallas as pl
from jax.experimental.pallas import tpu as pltpu
from jax.sharding import Mesh
from jax.sharding import PartitionSpec as P


HEADS = 16
KV_HEADS = 4
HEAD_DIM = 128
WINDOW = 128
BLOCK = 128
GROUP_EXPERTS = 3
GROUP_CAP = 10
LANES = 128
Z = "tp_0"
CORE = "tp_1"
TP = (Z, CORE)
SP_TP = ("sp", Z, CORE)
SWAP = [(0, 1), (1, 0)]

EPS = 1e-06
NEG_BIG = -1e30


def extended(block, width):
    count = lax.axis_size("sp")
    forward = [(i, i + 1) for i in range(count - 1)]
    backward = [(target, source) for source, target in forward]
    low = lax.ppermute(block[:, block.shape[1] - width :], "sp", forward)
    high = lax.ppermute(block[:, :width], "sp", backward)
    return jnp.concatenate([low, block, high], axis=1)


def chip_attention(queries, key_heads, value_heads, sink_logit):
    seq_rows = queries.shape[0]
    core = lax.axis_index(CORE)
    key_start = lax.axis_index(Z) * 2 * KV_HEADS // HEADS * HEAD_DIM
    key_own = lax.dynamic_slice_in_dim(key_heads, key_start, HEAD_DIM, 1)
    value_own = lax.dynamic_slice_in_dim(value_heads, key_start, HEAD_DIM, 1)
    padded = extended(jnp.stack([key_own, value_own]), WINDOW)
    blocks = seq_rows // (2 * BLOCK)
    query_blocks = queries.reshape(blocks, 2, BLOCK, HEAD_DIM)
    query_far = lax.ppermute(
        lax.dynamic_index_in_dim(query_blocks, 1 - core, 1, True), CORE, SWAP
    )
    query_pair = jnp.concatenate(
        [lax.dynamic_index_in_dim(query_blocks, core, 1, True), query_far], axis=1
    )
    sink_pair = jnp.concatenate([sink_logit, lax.ppermute(sink_logit, CORE, SWAP)])
    tile_rows = padded.reshape(2, 2 * blocks + 2, BLOCK, HEAD_DIM)
    key_spans = jnp.concatenate(
        [
            lax.dynamic_slice_in_dim(tile_rows, core + shifted, 2 * blocks - 1, 1)[:, ::2]
            for shifted in range(3)
        ],
        axis=2,
    )
    offset = lax.axis_index("sp") * seq_rows
    seq_total = seq_rows * lax.axis_size("sp")
    block_start = offset + (2 * jnp.arange(blocks, dtype=jnp.int32) + core) * BLOCK
    query_pos = block_start[:, None] + jnp.arange(BLOCK, dtype=jnp.int32)[None, :]
    key_pos = (
        block_start[:, None] + jnp.arange(BLOCK + 2 * WINDOW, dtype=jnp.int32)[None, :] - WINDOW
    )
    inside = (
        (jnp.abs(query_pos[:, :, None] - key_pos[:, None, :]) <= WINDOW)
        & (key_pos >= 0)[:, None, :]
        & (key_pos < seq_total)[:, None, :]
    )
    scores = jnp.einsum(
        "nhqd,nkd->nhqk", query_pair, key_spans[0], preferred_element_type=jnp.float32
    ) * HEAD_DIM ** (-0.5)
    scores = jnp.where(inside[:, None], scores, NEG_BIG)
    sink_col = sink_pair[None, :, None, None]
    row_top = jnp.maximum(jnp.max(scores, axis=3, keepdims=True), sink_col)
    exp_terms = jnp.exp(scores - row_top)
    row_mass = jnp.sum(exp_terms, axis=3, keepdims=True) + jnp.exp(sink_col - row_top)
    weight = (exp_terms / row_mass).astype(jnp.bfloat16)
    return jnp.einsum(
        "nhqk,nkd->nhqd", weight, key_spans[1], preferred_element_type=jnp.float32
    ).astype(jnp.bfloat16)


MAIN_CAP = 7
MAIN_COLS = 1280
REL = (0, -1, 1, -2, 2, -3, 3, 4)


def shifts():
    n = lax.axis_size(Z)
    up = [(i, (i + 1) % n) for i in range(n)]
    down = [(i, (i - 1) % n) for i in range(n)]
    return (lambda a: lax.ppermute(a, Z, up)), (lambda a: lax.ppermute(a, Z, down))


def ring_gather(block):
    up, down = shifts()
    half = block.shape[1] // (2 * LANES) * LANES
    blocks, low, high = [block], block, block
    for _ in range(3):
        low, high = up(low), down(high)
        blocks += [low, high]
    far = jnp.concatenate([up(low[:, :half]), down(high[:, half:])], axis=1)
    return blocks + [far]


def ring_reduce(parts):
    up, down = shifts()
    half = parts[0].shape[1] // 2
    low, high = up(parts[4][:, :half]), down(parts[4][:, half:])
    low = jnp.concatenate([parts[3][:, :half] + low, parts[3][:, half:]], axis=1)
    high = jnp.concatenate([parts[-3][:, :half], parts[-3][:, half:] + high], axis=1)
    for step in (2, 1):
        low, high = parts[step] + up(low), parts[-step] + down(high)
    return parts[0] + up(low) + down(high)


def in_ring_order(blocks, near_first):
    me = lax.axis_index(Z)
    n = lax.axis_size(Z)
    return [lax.dynamic_index_in_dim(blocks, (me + r) % n, 0, False) for r in near_first]


def experts_kernel(rows_in, *refs):
    weights_in, out_to = refs[:6], refs[6]
    weights, (rows, hidden, out) = refs[7:13], refs[13:16]
    weight_sems, row_sems, out_sems = refs[16:]
    gate_own, gate_far, up_own, up_far, down_own, down_far = weights
    total = rows.shape[0]
    width = out.shape[1]
    hid = 2 * gate_own.shape[2]
    steps = -(-total // 512)
    step = total // steps
    wide = 512

    def span(i):
        return pl.ds(pl.multiple_of(i * step, 16), step)

    def weight_copy(k, e):
        return pltpu.make_async_copy(weights_in[k].at[e], weights[k].at[e], weight_sems.at[k, e])

    def row_copy(i):
        return pltpu.make_async_copy(rows_in.at[span(i)], rows.at[span(i)], row_sems.at[i])

    def out_copy(i):
        return pltpu.make_async_copy(out.at[span(i)], out_to.at[span(i)], out_sems.at[i])

    for k in range(4):
        weight_copy(k, 0).start()
    for i in range(steps):
        row_copy(i).start()
    for e in range(1, GROUP_EXPERTS):
        for k in range(4):
            weight_copy(k, e).start()
    for e in range(GROUP_EXPERTS):
        for k in (4, 5):
            weight_copy(k, e).start()

    @pl.loop(0, GROUP_EXPERTS)
    def _(e):
        for k in range(4):
            weight_copy(k, e).wait()

        @pl.loop(0, steps)
        def _(i):
            @pl.when(e == 0)
            def _():
                row_copy(i).wait()

            joined = jnp.concatenate([gate_own[e], gate_far[e], up_own[e], up_far[e]], axis=1)
            both = jnp.dot(rows[span(i), :width], joined, preferred_element_type=jnp.float32)
            pre = both[:, :hid]
            gates = rows[span(i), width:].astype(jnp.float32)
            lane = lax.broadcasted_iota(jnp.int32, gates.shape, 1)
            gate = jnp.sum(jnp.where(lane == e, gates, 0.0), axis=1, keepdims=True)
            gated = pre / (1.0 + jnp.exp(-pre)) * both[:, hid:] * gate
            hidden[e, span(i), :] = gated.astype(jnp.bfloat16)

    for e in range(GROUP_EXPERTS):
        for k in (4, 5):
            weight_copy(k, e).wait()

    @pl.loop(0, steps)
    def _(i):
        joined = jnp.concatenate([hidden[e, span(i), :] for e in range(GROUP_EXPERTS)], axis=1)

        @pl.loop(0, width // wide)
        def _(c):
            cols = pl.ds(pl.multiple_of(c * wide, wide), wide)
            pieces = []
            for e in range(GROUP_EXPERTS):
                pieces += [down_own[e, :, cols], down_far[e, :, cols]]
            out[span(i), cols] = jnp.dot(
                joined, jnp.concatenate(pieces, axis=0), preferred_element_type=jnp.float32
            ).astype(jnp.bfloat16)

        out_copy(i).start()

    for i in range(steps):
        out_copy(i).wait()


def experts(rows, gate_pair, up_pair, down_pair):
    total, lanes = rows.shape
    width = lanes - LANES
    hid = gate_pair[0].shape[2]
    steps = -(-total // 512)
    work = total * width * hid * 2 * GROUP_EXPERTS
    anywhere = pl.BlockSpec(memory_space=pltpu.HBM)
    into = pltpu.VMEM((GROUP_EXPERTS, width, hid), jnp.bfloat16)
    outof = pltpu.VMEM((GROUP_EXPERTS, hid, width), jnp.bfloat16)
    return pl.pallas_call(
        experts_kernel,
        in_specs=[anywhere] * 7,
        out_specs=anywhere,
        out_shape=jax.ShapeDtypeStruct((total, width), jnp.bfloat16),
        scratch_shapes=[into] * 4
        + [outof] * 2
        + [
            pltpu.VMEM((total, lanes), jnp.bfloat16),
            pltpu.VMEM((GROUP_EXPERTS, total, 2 * hid), jnp.bfloat16),
            pltpu.VMEM((total, width), jnp.bfloat16),
            pltpu.SemaphoreType.DMA((6, GROUP_EXPERTS)),
            pltpu.SemaphoreType.DMA((steps,)),
            pltpu.SemaphoreType.DMA((steps,)),
        ],
        compiler_params=pltpu.CompilerParams(vmem_limit_bytes=62 * 2**20),
        cost_estimate=pl.CostEstimate(
            flops=6 * work, bytes_accessed=20 * 2**20, transcendentals=total * hid * 6
        ),
        name="experts",
    )(rows, *gate_pair, *up_pair, *down_pair)


def per_device(
    queries,
    key_heads,
    value_heads,
    sink_logit,
    out_weight,
    residual,
    mixer_gain,
    expert_gain,
    route_group,
    route_member,
    route_weight,
    gate_weight,
    up_weight,
    down_weight,
):
    groups = lax.axis_size("sp")
    width = residual.shape[1]
    capacity = GROUP_CAP
    slots = groups * capacity
    cap_a = MAIN_CAP
    cap_b = capacity - cap_a
    slots_b = groups * cap_b


    gate_pair, up_pair, down_pair = (
        (shard, lax.ppermute(shard, CORE, SWAP))
        for shard in (gate_weight, up_weight, down_weight)
    )

    group_ids = jnp.arange(groups, dtype=jnp.int32)
    chosen = (route_group[:, None] == group_ids[None, :]).astype(jnp.int32)
    group_rank = jnp.sum(chosen * (jnp.cumsum(chosen, axis=0) - 1), axis=1)
    slot_ids = route_group * capacity + group_rank
    placing = (jnp.arange(slots, dtype=jnp.int32)[:, None] == slot_ids[None, :]).astype(
        jnp.bfloat16
    )
    member_ids = jnp.arange(GROUP_EXPERTS, dtype=jnp.int32)
    token_gates = jnp.sum(
        route_weight.astype(jnp.float32)[:, :, None]
        * (route_member[:, :, None] == member_ids[None, None, :]).astype(jnp.float32),
        axis=1,
    ).astype(jnp.bfloat16)
    send_gates = jnp.dot(
        placing,
        jnp.pad(token_gates, ((0, 0), (0, LANES - GROUP_EXPERTS))),
        preferred_element_type=jnp.float32,
    ).astype(jnp.bfloat16)
    send_gates = jnp.pad(
        send_gates.reshape(groups, capacity, LANES), ((0, 0), (0, 16 - capacity), (0, 0))
    )

    weight_pair = jnp.stack([out_weight, lax.ppermute(out_weight, CORE, SWAP)])
    attended = chip_attention(queries, key_heads, value_heads, sink_logit)

    def head_part(cols):
        return jnp.einsum(
            "nhqd,hdm->nqm", attended, weight_pair[:, :, cols], preferred_element_type=jnp.float32
        ).astype(jnp.bfloat16)

    ring_part = head_part(slice(MAIN_COLS, width))
    main_part = head_part(slice(0, MAIN_COLS)).reshape(-1, MAIN_COLS)
    main_sum = lax.psum_scatter(main_part, Z, scatter_dimension=0, tiled=True)
    ring_sum = ring_reduce(dict(zip(REL, in_ring_order(ring_part, REL))))
    projected = jnp.concatenate([main_sum, ring_sum], axis=1).astype(jnp.float32)
    projected, gate_pair, up_pair, down_pair = lax.optimization_barrier(
        (projected, gate_pair, up_pair, down_pair)
    )

    proj_scale = lax.rsqrt(jnp.mean(projected * projected, axis=1, keepdims=True) + EPS)
    mixed_rows = (residual.astype(jnp.float32) + mixer_gain * (projected * proj_scale)).astype(
        jnp.bfloat16
    )
    mixed_float = mixed_rows.astype(jnp.float32)
    norm_scale = lax.rsqrt(jnp.mean(mixed_float * mixed_float, axis=1, keepdims=True) + EPS)
    normed = (mixed_float * norm_scale * expert_gain).astype(jnp.bfloat16)

    def exchange(rows):
        return lax.all_to_all(
            rows.reshape(groups, -1, LANES), "sp", split_axis=0, concat_axis=0, tiled=True
        )

    send_rows = jnp.dot(placing, normed, preferred_element_type=jnp.float32).astype(jnp.bfloat16)
    send_rows = send_rows.reshape(groups, capacity * width // LANES, LANES)
    tiles = width // LANES
    arrived = exchange(jnp.concatenate([send_rows, send_gates], axis=1))

    def with_gates(low, high):
        rows = arrived[:, low * tiles : high * tiles].reshape(-1, width)
        gates = arrived[:, capacity * tiles + low : capacity * tiles + high].reshape(-1, LANES)
        return jnp.concatenate([rows, gates], axis=1)

    pool_a = lax.all_gather(with_gates(0, cap_a), Z, axis=0, tiled=True)
    pool_b = ring_gather(with_gates(cap_a, capacity))
    part_b = experts(jnp.concatenate(pool_b, axis=0), gate_pair, up_pair, down_pair)
    pool_a, part_b = lax.optimization_barrier((pool_a, part_b))
    part_a = experts(pool_a, gate_pair, up_pair, down_pair)
    sum_a = lax.psum_scatter(part_a, Z, scatter_dimension=0, tiled=True)
    sum_b = ring_reduce(
        {r: part_b[k * slots_b : (k + 1) * slots_b] for k, r in enumerate(REL)}
    )
    back_b = exchange(sum_b)
    back_a = exchange(sum_a)
    returned = jnp.concatenate([back_a, back_b], axis=1).reshape(slots, width)
    expert_out = lax.dot_general(
        placing,
        returned,
        (((0,), (0,)), ((), ())),
        preferred_element_type=jnp.float32,
    )
    return (mixed_float + expert_out).astype(jnp.bfloat16)


def solution(mesh):
    torus = Mesh(mesh.devices.reshape(mesh.shape["sp"], 8, 2), ("sp", Z, CORE))
    placed = (
        P("sp", TP),
        P("sp", None),
        P("sp", None),
        P(TP),
        P(TP, None),
        P(SP_TP, None),
        P(),
        P(),
        P(SP_TP),
        P(SP_TP, None),
        P(SP_TP, None),
        P("sp", None, TP),
        P("sp", None, TP),
        P("sp", TP, None),
    )

    return jax.shard_map(
        per_device, mesh=torus, in_specs=placed, out_specs=P(SP_TP, None), check_vma=False
    )
```

```python
import jax
import jax.numpy as jnp
from jax import lax
from jax.experimental import pallas as pl
from jax.experimental.pallas import tpu as pltpu
from jax.sharding import Mesh
from jax.sharding import PartitionSpec as P


HEADS = 16
KV_HEADS = 4
HEAD_DIM = 128
WINDOW = 128
BLOCK = 128
GROUP_EXPERTS = 3
GROUP_CAP = 10
LANES = 128
Z = "tp_0"
CORE = "tp_1"
TP = (Z, CORE)
SP_TP = ("sp", Z, CORE)
SWAP = [(0, 1), (1, 0)]

EPS = 1e-06
NEG_BIG = -1e30


def extended(block, width):
    count = lax.axis_size("sp")
    forward = [(i, i + 1) for i in range(count - 1)]
    backward = [(target, source) for source, target in forward]
    low = lax.ppermute(block[:, block.shape[1] - width :], "sp", forward)
    high = lax.ppermute(block[:, :width], "sp", backward)
    return jnp.concatenate([low, block, high], axis=1)


def chip_attention(queries, key_heads, value_heads, sink_logit):
    seq_rows = queries.shape[0]
    core = lax.axis_index(CORE)
    key_start = lax.axis_index(Z) * 2 * KV_HEADS // HEADS * HEAD_DIM
    key_own = lax.dynamic_slice_in_dim(key_heads, key_start, HEAD_DIM, 1)
    value_own = lax.dynamic_slice_in_dim(value_heads, key_start, HEAD_DIM, 1)
    padded = extended(jnp.stack([key_own, value_own]), WINDOW)
    blocks = seq_rows // (2 * BLOCK)
    query_blocks = queries.reshape(blocks, 2, BLOCK, HEAD_DIM)
    query_far = lax.ppermute(
        lax.dynamic_index_in_dim(query_blocks, 1 - core, 1, True), CORE, SWAP
    )
    query_pair = jnp.concatenate(
        [lax.dynamic_index_in_dim(query_blocks, core, 1, True), query_far], axis=1
    )
    sink_pair = jnp.concatenate([sink_logit, lax.ppermute(sink_logit, CORE, SWAP)])
    tile_rows = padded.reshape(2, 2 * blocks + 2, BLOCK, HEAD_DIM)
    key_spans = jnp.concatenate(
        [
            lax.dynamic_slice_in_dim(tile_rows, core + shifted, 2 * blocks - 1, 1)[:, ::2]
            for shifted in range(3)
        ],
        axis=2,
    )
    offset = lax.axis_index("sp") * seq_rows
    seq_total = seq_rows * lax.axis_size("sp")
    block_start = offset + (2 * jnp.arange(blocks, dtype=jnp.int32) + core) * BLOCK
    query_pos = block_start[:, None] + jnp.arange(BLOCK, dtype=jnp.int32)[None, :]
    key_pos = (
        block_start[:, None] + jnp.arange(BLOCK + 2 * WINDOW, dtype=jnp.int32)[None, :] - WINDOW
    )
    inside = (
        (jnp.abs(query_pos[:, :, None] - key_pos[:, None, :]) <= WINDOW)
        & (key_pos >= 0)[:, None, :]
        & (key_pos < seq_total)[:, None, :]
    )
    scores = jnp.einsum(
        "nhqd,nkd->nhqk", query_pair, key_spans[0], preferred_element_type=jnp.float32
    ) * HEAD_DIM ** (-0.5)
    scores = jnp.where(inside[:, None], scores, NEG_BIG)
    sink_col = sink_pair[None, :, None, None]
    row_top = jnp.maximum(jnp.max(scores, axis=3, keepdims=True), sink_col)
    exp_terms = jnp.exp(scores - row_top)
    row_mass = jnp.sum(exp_terms, axis=3, keepdims=True) + jnp.exp(sink_col - row_top)
    weight = (exp_terms / row_mass).astype(jnp.bfloat16)
    return jnp.einsum(
        "nhqk,nkd->nhqd", weight, key_spans[1], preferred_element_type=jnp.float32
    ).astype(jnp.bfloat16)


MAIN_CAP = 7
MAIN_COLS = 1280
REL = (0, -1, 1, -2, 2, -3, 3, 4)


def shifts():
    n = lax.axis_size(Z)
    up = [(i, (i + 1) % n) for i in range(n)]
    down = [(i, (i - 1) % n) for i in range(n)]
    return (lambda a: lax.ppermute(a, Z, up)), (lambda a: lax.ppermute(a, Z, down))


def ring_gather(block):
    up, down = shifts()
    half = block.shape[1] // (2 * LANES) * LANES
    blocks, low, high = [block], block, block
    for _ in range(3):
        low, high = up(low), down(high)
        blocks += [low, high]
    far = jnp.concatenate([up(low[:, :half]), down(high[:, half:])], axis=1)
    return blocks + [far]


def ring_reduce(parts):
    up, down = shifts()
    half = parts[0].shape[1] // 2
    low, high = up(parts[4][:, :half]), down(parts[4][:, half:])
    low = jnp.concatenate([parts[3][:, :half] + low, parts[3][:, half:]], axis=1)
    high = jnp.concatenate([parts[-3][:, :half], parts[-3][:, half:] + high], axis=1)
    for step in (2, 1):
        low, high = parts[step] + up(low), parts[-step] + down(high)
    return parts[0] + up(low) + down(high)


def in_ring_order(blocks, near_first):
    me = lax.axis_index(Z)
    n = lax.axis_size(Z)
    return [lax.dynamic_index_in_dim(blocks, (me + r) % n, 0, False) for r in near_first]


def experts_kernel(rows_in, *refs):
    weights_in, out_to = refs[:6], refs[6]
    weights, (rows, hidden, out) = refs[7:13], refs[13:16]
    weight_sems, row_sems, out_sems = refs[16:]
    gate_own, gate_far, up_own, up_far, down_own, down_far = weights
    total = rows.shape[0]
    width = out.shape[1]
    hid = 2 * gate_own.shape[2]
    steps = -(-total // 512)
    step = total // steps
    wide = 512

    def span(i):
        start = i * step
        return pl.ds(start if isinstance(i, int) else pl.multiple_of(start, 16), step)

    def weight_copy(k, e):
        return pltpu.make_async_copy(weights_in[k].at[e], weights[k].at[e], weight_sems.at[k, e])

    def row_copy(i):
        return pltpu.make_async_copy(rows_in.at[span(i)], rows.at[span(i)], row_sems.at[i])

    def out_copy(i):
        return pltpu.make_async_copy(out.at[span(i)], out_to.at[span(i)], out_sems.at[i])

    for k in range(4):
        weight_copy(k, 0).start()
    for i in range(steps):
        row_copy(i).start()
    for e in range(1, GROUP_EXPERTS):
        for k in range(4):
            weight_copy(k, e).start()
    for e in range(GROUP_EXPERTS):
        for k in (4, 5):
            weight_copy(k, e).start()

    @pl.loop(0, GROUP_EXPERTS)
    def _(e):
        for k in range(4):
            weight_copy(k, e).wait()

        for i in range(steps):
            @pl.when(e == 0)
            def _(i=i):
                row_copy(i).wait()

            joined = jnp.concatenate([gate_own[e], gate_far[e], up_own[e], up_far[e]], axis=1)
            both = jnp.dot(rows[span(i), :width], joined, preferred_element_type=jnp.float32)
            pre = both[:, :hid]
            gates = rows[span(i), width:].astype(jnp.float32)
            lane = lax.broadcasted_iota(jnp.int32, gates.shape, 1)
            gate = jnp.sum(jnp.where(lane == e, gates, 0.0), axis=1, keepdims=True)
            gated = pre / (1.0 + jnp.exp(-pre)) * both[:, hid:] * gate
            hidden[e, span(i), :] = gated.astype(jnp.bfloat16)

    for e in range(GROUP_EXPERTS):
        for k in (4, 5):
            weight_copy(k, e).wait()

    @pl.loop(0, steps)
    def _(i):
        joined = jnp.concatenate([hidden[e, span(i), :] for e in range(GROUP_EXPERTS)], axis=1)

        @pl.loop(0, width // wide)
        def _(c):
            cols = pl.ds(pl.multiple_of(c * wide, wide), wide)
            pieces = []
            for e in range(GROUP_EXPERTS):
                pieces += [down_own[e, :, cols], down_far[e, :, cols]]
            out[span(i), cols] = jnp.dot(
                joined, jnp.concatenate(pieces, axis=0), preferred_element_type=jnp.float32
            ).astype(jnp.bfloat16)

        out_copy(i).start()

    for i in range(steps):
        out_copy(i).wait()


def experts(rows, gate_pair, up_pair, down_pair):
    total, lanes = rows.shape
    width = lanes - LANES
    hid = gate_pair[0].shape[2]
    steps = -(-total // 512)
    work = total * width * hid * 2 * GROUP_EXPERTS
    anywhere = pl.BlockSpec(memory_space=pltpu.HBM)
    into = pltpu.VMEM((GROUP_EXPERTS, width, hid), jnp.bfloat16)
    outof = pltpu.VMEM((GROUP_EXPERTS, hid, width), jnp.bfloat16)
    return pl.pallas_call(
        experts_kernel,
        in_specs=[anywhere] * 7,
        out_specs=anywhere,
        out_shape=jax.ShapeDtypeStruct((total, width), jnp.bfloat16),
        scratch_shapes=[into] * 4
        + [outof] * 2
        + [
            pltpu.VMEM((total, lanes), jnp.bfloat16),
            pltpu.VMEM((GROUP_EXPERTS, total, 2 * hid), jnp.bfloat16),
            pltpu.VMEM((total, width), jnp.bfloat16),
            pltpu.SemaphoreType.DMA((6, GROUP_EXPERTS)),
            pltpu.SemaphoreType.DMA((steps,)),
            pltpu.SemaphoreType.DMA((steps,)),
        ],
        compiler_params=pltpu.CompilerParams(vmem_limit_bytes=62 * 2**20),
        cost_estimate=pl.CostEstimate(
            flops=6 * work, bytes_accessed=20 * 2**20, transcendentals=total * hid * 6
        ),
        name="experts",
    )(rows, *gate_pair, *up_pair, *down_pair)


def per_device(
    queries,
    key_heads,
    value_heads,
    sink_logit,
    out_weight,
    residual,
    mixer_gain,
    expert_gain,
    route_group,
    route_member,
    route_weight,
    gate_weight,
    up_weight,
    down_weight,
):
    groups = lax.axis_size("sp")
    width = residual.shape[1]
    capacity = GROUP_CAP
    slots = groups * capacity
    cap_a = MAIN_CAP
    cap_b = capacity - cap_a
    slots_b = groups * cap_b


    gate_pair, up_pair, down_pair = (
        (shard, lax.ppermute(shard, CORE, SWAP))
        for shard in (gate_weight, up_weight, down_weight)
    )

    group_ids = jnp.arange(groups, dtype=jnp.int32)
    chosen = (route_group[:, None] == group_ids[None, :]).astype(jnp.int32)
    group_rank = jnp.sum(chosen * (jnp.cumsum(chosen, axis=0) - 1), axis=1)
    slot_ids = route_group * capacity + group_rank
    placing = (jnp.arange(slots, dtype=jnp.int32)[:, None] == slot_ids[None, :]).astype(
        jnp.bfloat16
    )
    member_ids = jnp.arange(GROUP_EXPERTS, dtype=jnp.int32)
    token_gates = jnp.sum(
        route_weight.astype(jnp.float32)[:, :, None]
        * (route_member[:, :, None] == member_ids[None, None, :]).astype(jnp.float32),
        axis=1,
    ).astype(jnp.bfloat16)
    send_gates = jnp.dot(
        placing,
        jnp.pad(token_gates, ((0, 0), (0, LANES - GROUP_EXPERTS))),
        preferred_element_type=jnp.float32,
    ).astype(jnp.bfloat16)
    send_gates = jnp.pad(
        send_gates.reshape(groups, capacity, LANES), ((0, 0), (0, 16 - capacity), (0, 0))
    )

    weight_pair = jnp.stack([out_weight, lax.ppermute(out_weight, CORE, SWAP)])
    attended = chip_attention(queries, key_heads, value_heads, sink_logit)

    def head_part(cols):
        return jnp.einsum(
            "nhqd,hdm->nqm", attended, weight_pair[:, :, cols], preferred_element_type=jnp.float32
        ).astype(jnp.bfloat16)

    ring_part = head_part(slice(MAIN_COLS, width))
    main_part = head_part(slice(0, MAIN_COLS)).reshape(-1, MAIN_COLS)
    main_sum = lax.psum_scatter(main_part, Z, scatter_dimension=0, tiled=True)
    ring_sum = ring_reduce(dict(zip(REL, in_ring_order(ring_part, REL))))
    projected = jnp.concatenate([main_sum, ring_sum], axis=1).astype(jnp.float32)
    projected, gate_pair, up_pair, down_pair = lax.optimization_barrier(
        (projected, gate_pair, up_pair, down_pair)
    )

    proj_scale = lax.rsqrt(jnp.mean(projected * projected, axis=1, keepdims=True) + EPS)
    mixed_rows = (residual.astype(jnp.float32) + mixer_gain * (projected * proj_scale)).astype(
        jnp.bfloat16
    )
    mixed_float = mixed_rows.astype(jnp.float32)
    norm_scale = lax.rsqrt(jnp.mean(mixed_float * mixed_float, axis=1, keepdims=True) + EPS)
    normed = (mixed_float * norm_scale * expert_gain).astype(jnp.bfloat16)

    def exchange(rows):
        return lax.all_to_all(
            rows.reshape(groups, -1, LANES), "sp", split_axis=0, concat_axis=0, tiled=True
        )

    send_rows = jnp.dot(placing, normed, preferred_element_type=jnp.float32).astype(jnp.bfloat16)
    send_rows = send_rows.reshape(groups, capacity * width // LANES, LANES)
    tiles = width // LANES
    arrived = exchange(jnp.concatenate([send_rows, send_gates], axis=1))

    def with_gates(low, high):
        rows = arrived[:, low * tiles : high * tiles].reshape(-1, width)
        gates = arrived[:, capacity * tiles + low : capacity * tiles + high].reshape(-1, LANES)
        return jnp.concatenate([rows, gates], axis=1)

    pool_a = lax.all_gather(with_gates(0, cap_a), Z, axis=0, tiled=True)
    pool_b = ring_gather(with_gates(cap_a, capacity))
    part_b = experts(jnp.concatenate(pool_b, axis=0), gate_pair, up_pair, down_pair)
    pool_a, part_b = lax.optimization_barrier((pool_a, part_b))
    part_a = experts(pool_a, gate_pair, up_pair, down_pair)
    sum_a = lax.psum_scatter(part_a, Z, scatter_dimension=0, tiled=True)
    sum_b = ring_reduce(
        {r: part_b[k * slots_b : (k + 1) * slots_b] for k, r in enumerate(REL)}
    )
    back_b = exchange(sum_b)
    back_a = exchange(sum_a)
    returned = jnp.concatenate([back_a, back_b], axis=1).reshape(slots, width)
    expert_out = lax.dot_general(
        placing,
        returned,
        (((0,), (0,)), ((), ())),
        preferred_element_type=jnp.float32,
    )
    return (mixed_float + expert_out).astype(jnp.bfloat16)


def solution(mesh):
    torus = Mesh(mesh.devices.reshape(mesh.shape["sp"], 8, 2), ("sp", Z, CORE))
    placed = (
        P("sp", TP),
        P("sp", None),
        P("sp", None),
        P(TP),
        P(TP, None),
        P(SP_TP, None),
        P(),
        P(),
        P(SP_TP),
        P(SP_TP, None),
        P(SP_TP, None),
        P("sp", None, TP),
        P("sp", None, TP),
        P("sp", TP, None),
    )

    return jax.shard_map(
        per_device, mesh=torus, in_specs=placed, out_specs=P(SP_TP, None), check_vma=False
    )
```

```python
import jax
import jax.numpy as jnp
from jax import lax
from jax.experimental import pallas as pl
from jax.experimental.pallas import tpu as pltpu
from jax.sharding import Mesh
from jax.sharding import PartitionSpec as P


HEADS = 16
KV_HEADS = 4
HEAD_DIM = 128
WINDOW = 128
BLOCK = 128
GROUP_EXPERTS = 3
GROUP_CAP = 10
LANES = 128
Z = "tp_0"
CORE = "tp_1"
TP = (Z, CORE)
SP_TP = ("sp", Z, CORE)
SWAP = [(0, 1), (1, 0)]

EPS = 1e-06
NEG_BIG = -1e30


def extended(block, width):
    count = lax.axis_size("sp")
    forward = [(i, i + 1) for i in range(count - 1)]
    backward = [(target, source) for source, target in forward]
    low = lax.ppermute(block[:, block.shape[1] - width :], "sp", forward)
    high = lax.ppermute(block[:, :width], "sp", backward)
    return jnp.concatenate([low, block, high], axis=1)


def chip_attention(queries, key_heads, value_heads, sink_logit):
    seq_rows = queries.shape[0]
    core = lax.axis_index(CORE)
    key_start = lax.axis_index(Z) * 2 * KV_HEADS // HEADS * HEAD_DIM
    key_own = lax.dynamic_slice_in_dim(key_heads, key_start, HEAD_DIM, 1)
    value_own = lax.dynamic_slice_in_dim(value_heads, key_start, HEAD_DIM, 1)
    padded = extended(jnp.stack([key_own, value_own]), WINDOW)
    blocks = seq_rows // (2 * BLOCK)
    query_blocks = queries.reshape(blocks, 2, BLOCK, HEAD_DIM)
    query_far = lax.ppermute(
        lax.dynamic_index_in_dim(query_blocks, 1 - core, 1, True), CORE, SWAP
    )
    query_pair = jnp.concatenate(
        [lax.dynamic_index_in_dim(query_blocks, core, 1, True), query_far], axis=1
    )
    sink_pair = jnp.concatenate([sink_logit, lax.ppermute(sink_logit, CORE, SWAP)])
    tile_rows = padded.reshape(2, 2 * blocks + 2, BLOCK, HEAD_DIM)
    key_spans = jnp.concatenate(
        [
            lax.dynamic_slice_in_dim(tile_rows, core + shifted, 2 * blocks - 1, 1)[:, ::2]
            for shifted in range(3)
        ],
        axis=2,
    )
    offset = lax.axis_index("sp") * seq_rows
    seq_total = seq_rows * lax.axis_size("sp")
    block_start = offset + (2 * jnp.arange(blocks, dtype=jnp.int32) + core) * BLOCK
    query_pos = block_start[:, None] + jnp.arange(BLOCK, dtype=jnp.int32)[None, :]
    key_pos = (
        block_start[:, None] + jnp.arange(BLOCK + 2 * WINDOW, dtype=jnp.int32)[None, :] - WINDOW
    )
    inside = (
        (jnp.abs(query_pos[:, :, None] - key_pos[:, None, :]) <= WINDOW)
        & (key_pos >= 0)[:, None, :]
        & (key_pos < seq_total)[:, None, :]
    )
    scores = jnp.einsum(
        "nhqd,nkd->nhqk", query_pair, key_spans[0], preferred_element_type=jnp.float32
    ) * HEAD_DIM ** (-0.5)
    scores = jnp.where(inside[:, None], scores, NEG_BIG)
    sink_col = sink_pair[None, :, None, None]
    row_top = jnp.maximum(jnp.max(scores, axis=3, keepdims=True), sink_col)
    exp_terms = jnp.exp(scores - row_top)
    row_mass = jnp.sum(exp_terms, axis=3, keepdims=True) + jnp.exp(sink_col - row_top)
    weight = (exp_terms / row_mass).astype(jnp.bfloat16)
    return jnp.einsum(
        "nhqk,nkd->nhqd", weight, key_spans[1], preferred_element_type=jnp.float32
    ).astype(jnp.bfloat16)


MAIN_CAP = 7
MAIN_COLS = 1280
REL = (0, -1, 1, -2, 2, -3, 3, 4)


def shifts():
    n = lax.axis_size(Z)
    up = [(i, (i + 1) % n) for i in range(n)]
    down = [(i, (i - 1) % n) for i in range(n)]
    return (lambda a: lax.ppermute(a, Z, up)), (lambda a: lax.ppermute(a, Z, down))


def ring_gather(block):
    up, down = shifts()
    half = block.shape[1] // (2 * LANES) * LANES
    blocks, low, high = [block], block, block
    for _ in range(3):
        low, high = up(low), down(high)
        blocks += [low, high]
    far = jnp.concatenate([up(low[:, :half]), down(high[:, half:])], axis=1)
    return blocks + [far]


def ring_reduce(parts):
    up, down = shifts()
    half = parts[0].shape[1] // 2
    low, high = up(parts[4][:, :half]), down(parts[4][:, half:])
    low = jnp.concatenate([parts[3][:, :half] + low, parts[3][:, half:]], axis=1)
    high = jnp.concatenate([parts[-3][:, :half], parts[-3][:, half:] + high], axis=1)
    for step in (2, 1):
        low, high = parts[step] + up(low), parts[-step] + down(high)
    return parts[0] + up(low) + down(high)


def in_ring_order(blocks, near_first):
    me = lax.axis_index(Z)
    n = lax.axis_size(Z)
    return [lax.dynamic_index_in_dim(blocks, (me + r) % n, 0, False) for r in near_first]


def experts_kernel(rows_in, *refs):
    weights_in, out_to = refs[:6], refs[6]
    weights, (rows, hidden, out) = refs[7:13], refs[13:16]
    weight_sems, row_sems, out_sems = refs[16:]
    gate_own, gate_far, up_own, up_far, down_own, down_far = weights
    total = rows.shape[0]
    width = out.shape[1]
    hid = 2 * gate_own.shape[2]
    steps = -(-total // 512)
    step = total // steps
    wide = 512

    def span(i):
        return pl.ds(pl.multiple_of(i * step, 16), step)

    def weight_copy(k, e):
        return pltpu.make_async_copy(weights_in[k].at[e], weights[k].at[e], weight_sems.at[k, e])

    def row_copy(i):
        return pltpu.make_async_copy(rows_in.at[span(i)], rows.at[span(i)], row_sems.at[i])

    def out_copy(i):
        return pltpu.make_async_copy(out.at[span(i)], out_to.at[span(i)], out_sems.at[i])

    row_copy(0).start()
    for k in range(4):
        weight_copy(k, 0).start()

    @pl.loop(0, GROUP_EXPERTS)
    def _(e):
        for k in range(4):
            weight_copy(k, e).wait()

        @pl.when(e == 0)
        def _():
            for i in range(1, steps):
                row_copy(i).start()

        @pl.when(e + 1 < GROUP_EXPERTS)
        def _():
            for k in range(4):
                weight_copy(k, e + 1).start()

        @pl.when(e == 1)
        def _():
            for member in range(GROUP_EXPERTS):
                for k in (4, 5):
                    weight_copy(k, member).start()

        @pl.loop(0, steps)
        def _(i):
            @pl.when(e == 0)
            def _():
                row_copy(i).wait()

            joined = jnp.concatenate([gate_own[e], gate_far[e], up_own[e], up_far[e]], axis=1)
            both = jnp.dot(rows[span(i), :width], joined, preferred_element_type=jnp.float32)
            pre = both[:, :hid]
            gates = rows[span(i), width:].astype(jnp.float32)
            lane = lax.broadcasted_iota(jnp.int32, gates.shape, 1)
            gate = jnp.sum(jnp.where(lane == e, gates, 0.0), axis=1, keepdims=True)
            gated = pre / (1.0 + jnp.exp(-pre)) * both[:, hid:] * gate
            hidden[e, span(i), :] = gated.astype(jnp.bfloat16)

    for e in range(GROUP_EXPERTS):
        for k in (4, 5):
            weight_copy(k, e).wait()

    @pl.loop(0, steps)
    def _(i):
        joined = jnp.concatenate([hidden[e, span(i), :] for e in range(GROUP_EXPERTS)], axis=1)

        @pl.loop(0, width // wide)
        def _(c):
            cols = pl.ds(pl.multiple_of(c * wide, wide), wide)
            pieces = []
            for e in range(GROUP_EXPERTS):
                pieces += [down_own[e, :, cols], down_far[e, :, cols]]
            out[span(i), cols] = jnp.dot(
                joined, jnp.concatenate(pieces, axis=0), preferred_element_type=jnp.float32
            ).astype(jnp.bfloat16)

        out_copy(i).start()

    for i in range(steps):
        out_copy(i).wait()


def experts(rows, gate_pair, up_pair, down_pair):
    total, lanes = rows.shape
    width = lanes - LANES
    hid = gate_pair[0].shape[2]
    steps = -(-total // 512)
    work = total * width * hid * 2 * GROUP_EXPERTS
    anywhere = pl.BlockSpec(memory_space=pltpu.HBM)
    into = pltpu.VMEM((GROUP_EXPERTS, width, hid), jnp.bfloat16)
    outof = pltpu.VMEM((GROUP_EXPERTS, hid, width), jnp.bfloat16)
    return pl.pallas_call(
        experts_kernel,
        in_specs=[anywhere] * 7,
        out_specs=anywhere,
        out_shape=jax.ShapeDtypeStruct((total, width), jnp.bfloat16),
        scratch_shapes=[into] * 4
        + [outof] * 2
        + [
            pltpu.VMEM((total, lanes), jnp.bfloat16),
            pltpu.VMEM((GROUP_EXPERTS, total, 2 * hid), jnp.bfloat16),
            pltpu.VMEM((total, width), jnp.bfloat16),
            pltpu.SemaphoreType.DMA((6, GROUP_EXPERTS)),
            pltpu.SemaphoreType.DMA((steps,)),
            pltpu.SemaphoreType.DMA((steps,)),
        ],
        compiler_params=pltpu.CompilerParams(vmem_limit_bytes=62 * 2**20),
        cost_estimate=pl.CostEstimate(
            flops=6 * work, bytes_accessed=20 * 2**20, transcendentals=total * hid * 6
        ),
        name="experts",
    )(rows, *gate_pair, *up_pair, *down_pair)


def per_device(
    queries,
    key_heads,
    value_heads,
    sink_logit,
    out_weight,
    residual,
    mixer_gain,
    expert_gain,
    route_group,
    route_member,
    route_weight,
    gate_weight,
    up_weight,
    down_weight,
):
    groups = lax.axis_size("sp")
    width = residual.shape[1]
    capacity = GROUP_CAP
    slots = groups * capacity
    cap_a = MAIN_CAP
    cap_b = capacity - cap_a
    slots_b = groups * cap_b


    gate_pair, up_pair, down_pair = (
        (shard, lax.ppermute(shard, CORE, SWAP))
        for shard in (gate_weight, up_weight, down_weight)
    )

    group_ids = jnp.arange(groups, dtype=jnp.int32)
    chosen = (route_group[:, None] == group_ids[None, :]).astype(jnp.int32)
    group_rank = jnp.sum(chosen * (jnp.cumsum(chosen, axis=0) - 1), axis=1)
    slot_ids = route_group * capacity + group_rank
    placing = (jnp.arange(slots, dtype=jnp.int32)[:, None] == slot_ids[None, :]).astype(
        jnp.bfloat16
    )
    member_ids = jnp.arange(GROUP_EXPERTS, dtype=jnp.int32)
    token_gates = jnp.sum(
        route_weight.astype(jnp.float32)[:, :, None]
        * (route_member[:, :, None] == member_ids[None, None, :]).astype(jnp.float32),
        axis=1,
    ).astype(jnp.bfloat16)
    send_gates = jnp.dot(
        placing,
        jnp.pad(token_gates, ((0, 0), (0, LANES - GROUP_EXPERTS))),
        preferred_element_type=jnp.float32,
    ).astype(jnp.bfloat16)
    send_gates = jnp.pad(
        send_gates.reshape(groups, capacity, LANES), ((0, 0), (0, 16 - capacity), (0, 0))
    )

    weight_pair = jnp.stack([out_weight, lax.ppermute(out_weight, CORE, SWAP)])
    attended = chip_attention(queries, key_heads, value_heads, sink_logit)

    def head_part(cols):
        return jnp.einsum(
            "nhqd,hdm->nqm", attended, weight_pair[:, :, cols], preferred_element_type=jnp.float32
        ).astype(jnp.bfloat16)

    ring_part = head_part(slice(MAIN_COLS, width))
    main_part = head_part(slice(0, MAIN_COLS)).reshape(-1, MAIN_COLS)
    main_sum = lax.psum_scatter(main_part, Z, scatter_dimension=0, tiled=True)
    ring_sum = ring_reduce(dict(zip(REL, in_ring_order(ring_part, REL))))
    projected = jnp.concatenate([main_sum, ring_sum], axis=1).astype(jnp.float32)
    projected, gate_pair, up_pair, down_pair = lax.optimization_barrier(
        (projected, gate_pair, up_pair, down_pair)
    )

    proj_scale = lax.rsqrt(jnp.mean(projected * projected, axis=1, keepdims=True) + EPS)
    mixed_rows = (residual.astype(jnp.float32) + mixer_gain * (projected * proj_scale)).astype(
        jnp.bfloat16
    )
    mixed_float = mixed_rows.astype(jnp.float32)
    norm_scale = lax.rsqrt(jnp.mean(mixed_float * mixed_float, axis=1, keepdims=True) + EPS)
    normed = (mixed_float * norm_scale * expert_gain).astype(jnp.bfloat16)

    def exchange(rows):
        return lax.all_to_all(
            rows.reshape(groups, -1, LANES), "sp", split_axis=0, concat_axis=0, tiled=True
        )

    send_rows = jnp.dot(placing, normed, preferred_element_type=jnp.float32).astype(jnp.bfloat16)
    send_rows = send_rows.reshape(groups, capacity * width // LANES, LANES)
    tiles = width // LANES
    arrived = exchange(jnp.concatenate([send_rows, send_gates], axis=1))

    def with_gates(low, high):
        rows = arrived[:, low * tiles : high * tiles].reshape(-1, width)
        gates = arrived[:, capacity * tiles + low : capacity * tiles + high].reshape(-1, LANES)
        return jnp.concatenate([rows, gates], axis=1)

    pool_a = lax.all_gather(with_gates(0, cap_a), Z, axis=0, tiled=True)
    pool_b = ring_gather(with_gates(cap_a, capacity))
    part_b = experts(jnp.concatenate(pool_b, axis=0), gate_pair, up_pair, down_pair)
    pool_a, part_b = lax.optimization_barrier((pool_a, part_b))
    part_a = experts(pool_a, gate_pair, up_pair, down_pair)
    sum_a = lax.psum_scatter(part_a, Z, scatter_dimension=0, tiled=True)
    sum_b = ring_reduce(
        {r: part_b[k * slots_b : (k + 1) * slots_b] for k, r in enumerate(REL)}
    )
    back_b = exchange(sum_b)
    back_a = exchange(sum_a)
    returned = jnp.concatenate([back_a, back_b], axis=1).reshape(slots, width)
    expert_out = lax.dot_general(
        placing,
        returned,
        (((0,), (0,)), ((), ())),
        preferred_element_type=jnp.float32,
    )
    return (mixed_float + expert_out).astype(jnp.bfloat16)


def solution(mesh):
    torus = Mesh(mesh.devices.reshape(mesh.shape["sp"], 8, 2), ("sp", Z, CORE))
    placed = (
        P("sp", TP),
        P("sp", None),
        P("sp", None),
        P(TP),
        P(TP, None),
        P(SP_TP, None),
        P(),
        P(),
        P(SP_TP),
        P(SP_TP, None),
        P(SP_TP, None),
        P("sp", None, TP),
        P("sp", None, TP),
        P("sp", TP, None),
    )

    return jax.shard_map(
        per_device, mesh=torus, in_specs=placed, out_specs=P(SP_TP, None), check_vma=False
    )
```

```python
import jax
import jax.numpy as jnp
from jax import lax
from jax.experimental import pallas as pl
from jax.experimental.pallas import tpu as pltpu
from jax.sharding import Mesh
from jax.sharding import PartitionSpec as P


HEADS = 16
KV_HEADS = 4
HEAD_DIM = 128
WINDOW = 128
BLOCK = 128
GROUP_EXPERTS = 3
GROUP_CAP = 10
LANES = 128
Z = "tp_0"
CORE = "tp_1"
TP = (Z, CORE)
SP_TP = ("sp", Z, CORE)
SWAP = [(0, 1), (1, 0)]

EPS = 1e-06
NEG_BIG = -1e30


def extended(block, width):
    count = lax.axis_size("sp")
    forward = [(i, i + 1) for i in range(count - 1)]
    backward = [(target, source) for source, target in forward]
    low = lax.ppermute(block[:, block.shape[1] - width :], "sp", forward)
    high = lax.ppermute(block[:, :width], "sp", backward)
    return jnp.concatenate([low, block, high], axis=1)


def chip_attention(queries, key_heads, value_heads, sink_logit):
    seq_rows = queries.shape[0]
    core = lax.axis_index(CORE)
    key_start = lax.axis_index(Z) * 2 * KV_HEADS // HEADS * HEAD_DIM
    key_own = lax.dynamic_slice_in_dim(key_heads, key_start, HEAD_DIM, 1)
    value_own = lax.dynamic_slice_in_dim(value_heads, key_start, HEAD_DIM, 1)
    padded = extended(jnp.stack([key_own, value_own]), WINDOW)
    blocks = seq_rows // (2 * BLOCK)
    query_blocks = queries.reshape(blocks, 2, BLOCK, HEAD_DIM)
    query_far = lax.ppermute(
        lax.dynamic_index_in_dim(query_blocks, 1 - core, 1, True), CORE, SWAP
    )
    query_pair = jnp.concatenate(
        [lax.dynamic_index_in_dim(query_blocks, core, 1, True), query_far], axis=1
    )
    sink_pair = jnp.concatenate([sink_logit, lax.ppermute(sink_logit, CORE, SWAP)])
    tile_rows = padded.reshape(2, 2 * blocks + 2, BLOCK, HEAD_DIM)
    key_spans = jnp.concatenate(
        [
            lax.dynamic_slice_in_dim(tile_rows, core + shifted, 2 * blocks - 1, 1)[:, ::2]
            for shifted in range(3)
        ],
        axis=2,
    )
    offset = lax.axis_index("sp") * seq_rows
    seq_total = seq_rows * lax.axis_size("sp")
    block_start = offset + (2 * jnp.arange(blocks, dtype=jnp.int32) + core) * BLOCK
    query_pos = block_start[:, None] + jnp.arange(BLOCK, dtype=jnp.int32)[None, :]
    key_pos = (
        block_start[:, None] + jnp.arange(BLOCK + 2 * WINDOW, dtype=jnp.int32)[None, :] - WINDOW
    )
    inside = (
        (jnp.abs(query_pos[:, :, None] - key_pos[:, None, :]) <= WINDOW)
        & (key_pos >= 0)[:, None, :]
        & (key_pos < seq_total)[:, None, :]
    )
    scores = jnp.einsum(
        "nhqd,nkd->nhqk", query_pair, key_spans[0], preferred_element_type=jnp.float32
    ) * HEAD_DIM ** (-0.5)
    scores = jnp.where(inside[:, None], scores, NEG_BIG)
    sink_col = sink_pair[None, :, None, None]
    row_top = jnp.maximum(jnp.max(scores, axis=3, keepdims=True), sink_col)
    exp_terms = jnp.exp(scores - row_top)
    row_mass = jnp.sum(exp_terms, axis=3, keepdims=True) + jnp.exp(sink_col - row_top)
    weight = (exp_terms / row_mass).astype(jnp.bfloat16)
    return jnp.einsum(
        "nhqk,nkd->nhqd", weight, key_spans[1], preferred_element_type=jnp.float32
    ).astype(jnp.bfloat16)


MAIN_CAP = 7
MAIN_COLS = 1280
REL = (0, -1, 1, -2, 2, -3, 3, 4)


def shifts():
    n = lax.axis_size(Z)
    up = [(i, (i + 1) % n) for i in range(n)]
    down = [(i, (i - 1) % n) for i in range(n)]
    return (lambda a: lax.ppermute(a, Z, up)), (lambda a: lax.ppermute(a, Z, down))


def ring_gather(block):
    up, down = shifts()
    half = block.shape[1] // (2 * LANES) * LANES
    blocks, low, high = [block], block, block
    for _ in range(3):
        low, high = up(low), down(high)
        blocks += [low, high]
    far = jnp.concatenate([up(low[:, :half]), down(high[:, half:])], axis=1)
    return blocks + [far]


def ring_reduce(parts):
    up, down = shifts()
    half = parts[0].shape[1] // 2
    low, high = up(parts[4][:, :half]), down(parts[4][:, half:])
    low = jnp.concatenate([parts[3][:, :half] + low, parts[3][:, half:]], axis=1)
    high = jnp.concatenate([parts[-3][:, :half], parts[-3][:, half:] + high], axis=1)
    for step in (2, 1):
        low, high = parts[step] + up(low), parts[-step] + down(high)
    return parts[0] + up(low) + down(high)


def in_ring_order(blocks, near_first):
    me = lax.axis_index(Z)
    n = lax.axis_size(Z)
    return [lax.dynamic_index_in_dim(blocks, (me + r) % n, 0, False) for r in near_first]


def experts_kernel(rows_in, *refs):
    weights_in, out_to = refs[:6], refs[6]
    weights, (rows, hidden, out) = refs[7:13], refs[13:16]
    weight_sems, row_sems, out_sems = refs[16:]
    gate_own, gate_far, up_own, up_far, down_own, down_far = weights
    total = rows.shape[0]
    width = out.shape[1]
    hid = 2 * gate_own.shape[2]
    steps = -(-total // 512)
    step = total // steps
    wide = 512

    def span(i):
        return pl.ds(pl.multiple_of(i * step, 16), step)

    def weight_copy(k, e):
        return pltpu.make_async_copy(weights_in[k].at[e], weights[k].at[e], weight_sems.at[k, e])

    def row_copy(i):
        return pltpu.make_async_copy(rows_in.at[span(i)], rows.at[span(i)], row_sems.at[i])

    def columns(c):
        return pl.ds(pl.multiple_of(c * wide, wide), wide)

    def out_copy(i, c):
        at = (span(i), columns(c))
        return pltpu.make_async_copy(out.at[at], out_to.at[at], out_sems.at[i, c])

    row_copy(0).start()
    for k in range(4):
        weight_copy(k, 0).start()

    @pl.loop(0, GROUP_EXPERTS)
    def _(e):
        for k in range(4):
            weight_copy(k, e).wait()

        @pl.when(e == 0)
        def _():
            for i in range(1, steps):
                row_copy(i).start()

        @pl.when(e + 1 < GROUP_EXPERTS)
        def _():
            for k in range(4):
                weight_copy(k, e + 1).start()

        @pl.when(e == 1)
        def _():
            for member in range(GROUP_EXPERTS):
                for k in (4, 5):
                    weight_copy(k, member).start()

        @pl.loop(0, steps)
        def _(i):
            @pl.when(e == 0)
            def _():
                row_copy(i).wait()

            joined = jnp.concatenate([gate_own[e], gate_far[e], up_own[e], up_far[e]], axis=1)
            both = jnp.dot(rows[span(i), :width], joined, preferred_element_type=jnp.float32)
            pre = both[:, :hid]
            gates = rows[span(i), width:].astype(jnp.float32)
            lane = lax.broadcasted_iota(jnp.int32, gates.shape, 1)
            gate = jnp.sum(jnp.where(lane == e, gates, 0.0), axis=1, keepdims=True)
            gated = pre / (1.0 + jnp.exp(-pre)) * both[:, hid:] * gate
            hidden[e, span(i), :] = gated.astype(jnp.bfloat16)

    for e in range(GROUP_EXPERTS):
        for k in (4, 5):
            weight_copy(k, e).wait()

    @pl.loop(0, steps)
    def _(i):
        joined = jnp.concatenate([hidden[e, span(i), :] for e in range(GROUP_EXPERTS)], axis=1)

        @pl.loop(0, width // wide)
        def _(c):
            cols = columns(c)
            pieces = []
            for e in range(GROUP_EXPERTS):
                pieces += [down_own[e, :, cols], down_far[e, :, cols]]
            out[span(i), cols] = jnp.dot(
                joined, jnp.concatenate(pieces, axis=0), preferred_element_type=jnp.float32
            ).astype(jnp.bfloat16)
            out_copy(i, c).start()

    for i in range(steps):
        for c in range(width // wide):
            out_copy(i, c).wait()


def experts(rows, gate_pair, up_pair, down_pair):
    total, lanes = rows.shape
    width = lanes - LANES
    hid = gate_pair[0].shape[2]
    steps = -(-total // 512)
    work = total * width * hid * 2 * GROUP_EXPERTS
    anywhere = pl.BlockSpec(memory_space=pltpu.HBM)
    into = pltpu.VMEM((GROUP_EXPERTS, width, hid), jnp.bfloat16)
    outof = pltpu.VMEM((GROUP_EXPERTS, hid, width), jnp.bfloat16)
    return pl.pallas_call(
        experts_kernel,
        in_specs=[anywhere] * 7,
        out_specs=anywhere,
        out_shape=jax.ShapeDtypeStruct((total, width), jnp.bfloat16),
        scratch_shapes=[into] * 4
        + [outof] * 2
        + [
            pltpu.VMEM((total, lanes), jnp.bfloat16),
            pltpu.VMEM((GROUP_EXPERTS, total, 2 * hid), jnp.bfloat16),
            pltpu.VMEM((total, width), jnp.bfloat16),
            pltpu.SemaphoreType.DMA((6, GROUP_EXPERTS)),
            pltpu.SemaphoreType.DMA((steps,)),
            pltpu.SemaphoreType.DMA((steps, width // 512)),
        ],
        compiler_params=pltpu.CompilerParams(vmem_limit_bytes=62 * 2**20),
        cost_estimate=pl.CostEstimate(
            flops=6 * work, bytes_accessed=20 * 2**20, transcendentals=total * hid * 6
        ),
        name="experts",
    )(rows, *gate_pair, *up_pair, *down_pair)


def per_device(
    queries,
    key_heads,
    value_heads,
    sink_logit,
    out_weight,
    residual,
    mixer_gain,
    expert_gain,
    route_group,
    route_member,
    route_weight,
    gate_weight,
    up_weight,
    down_weight,
):
    groups = lax.axis_size("sp")
    width = residual.shape[1]
    capacity = GROUP_CAP
    slots = groups * capacity
    cap_a = MAIN_CAP
    cap_b = capacity - cap_a
    slots_b = groups * cap_b


    gate_pair, up_pair, down_pair = (
        (shard, lax.ppermute(shard, CORE, SWAP))
        for shard in (gate_weight, up_weight, down_weight)
    )

    group_ids = jnp.arange(groups, dtype=jnp.int32)
    chosen = (route_group[:, None] == group_ids[None, :]).astype(jnp.int32)
    group_rank = jnp.sum(chosen * (jnp.cumsum(chosen, axis=0) - 1), axis=1)
    slot_ids = route_group * capacity + group_rank
    placing = (jnp.arange(slots, dtype=jnp.int32)[:, None] == slot_ids[None, :]).astype(
        jnp.bfloat16
    )
    member_ids = jnp.arange(GROUP_EXPERTS, dtype=jnp.int32)
    token_gates = jnp.sum(
        route_weight.astype(jnp.float32)[:, :, None]
        * (route_member[:, :, None] == member_ids[None, None, :]).astype(jnp.float32),
        axis=1,
    ).astype(jnp.bfloat16)
    send_gates = jnp.dot(
        placing,
        jnp.pad(token_gates, ((0, 0), (0, LANES - GROUP_EXPERTS))),
        preferred_element_type=jnp.float32,
    ).astype(jnp.bfloat16)
    send_gates = jnp.pad(
        send_gates.reshape(groups, capacity, LANES), ((0, 0), (0, 16 - capacity), (0, 0))
    )

    weight_pair = jnp.stack([out_weight, lax.ppermute(out_weight, CORE, SWAP)])
    attended = chip_attention(queries, key_heads, value_heads, sink_logit)

    def head_part(cols):
        return jnp.einsum(
            "nhqd,hdm->nqm", attended, weight_pair[:, :, cols], preferred_element_type=jnp.float32
        ).astype(jnp.bfloat16)

    ring_part = head_part(slice(MAIN_COLS, width))
    main_part = head_part(slice(0, MAIN_COLS)).reshape(-1, MAIN_COLS)
    main_sum = lax.psum_scatter(main_part, Z, scatter_dimension=0, tiled=True)
    ring_sum = ring_reduce(dict(zip(REL, in_ring_order(ring_part, REL))))
    projected = jnp.concatenate([main_sum, ring_sum], axis=1).astype(jnp.float32)
    projected, gate_pair, up_pair, down_pair = lax.optimization_barrier(
        (projected, gate_pair, up_pair, down_pair)
    )

    proj_scale = lax.rsqrt(jnp.mean(projected * projected, axis=1, keepdims=True) + EPS)
    mixed_rows = (residual.astype(jnp.float32) + mixer_gain * (projected * proj_scale)).astype(
        jnp.bfloat16
    )
    mixed_float = mixed_rows.astype(jnp.float32)
    norm_scale = lax.rsqrt(jnp.mean(mixed_float * mixed_float, axis=1, keepdims=True) + EPS)
    normed = (mixed_float * norm_scale * expert_gain).astype(jnp.bfloat16)

    def exchange(rows):
        return lax.all_to_all(
            rows.reshape(groups, -1, LANES), "sp", split_axis=0, concat_axis=0, tiled=True
        )

    send_rows = jnp.dot(placing, normed, preferred_element_type=jnp.float32).astype(jnp.bfloat16)
    send_rows = send_rows.reshape(groups, capacity * width // LANES, LANES)
    tiles = width // LANES
    arrived = exchange(jnp.concatenate([send_rows, send_gates], axis=1))

    def with_gates(low, high):
        rows = arrived[:, low * tiles : high * tiles].reshape(-1, width)
        gates = arrived[:, capacity * tiles + low : capacity * tiles + high].reshape(-1, LANES)
        return jnp.concatenate([rows, gates], axis=1)

    pool_a = lax.all_gather(with_gates(0, cap_a), Z, axis=0, tiled=True)
    pool_b = ring_gather(with_gates(cap_a, capacity))
    part_b = experts(jnp.concatenate(pool_b, axis=0), gate_pair, up_pair, down_pair)
    pool_a, part_b = lax.optimization_barrier((pool_a, part_b))
    part_a = experts(pool_a, gate_pair, up_pair, down_pair)
    sum_a = lax.psum_scatter(part_a, Z, scatter_dimension=0, tiled=True)
    sum_b = ring_reduce(
        {r: part_b[k * slots_b : (k + 1) * slots_b] for k, r in enumerate(REL)}
    )
    back_b = exchange(sum_b)
    back_a = exchange(sum_a)
    returned = jnp.concatenate([back_a, back_b], axis=1).reshape(slots, width)
    expert_out = lax.dot_general(
        placing,
        returned,
        (((0,), (0,)), ((), ())),
        preferred_element_type=jnp.float32,
    )
    return (mixed_float + expert_out).astype(jnp.bfloat16)


def solution(mesh):
    torus = Mesh(mesh.devices.reshape(mesh.shape["sp"], 8, 2), ("sp", Z, CORE))
    placed = (
        P("sp", TP),
        P("sp", None),
        P("sp", None),
        P(TP),
        P(TP, None),
        P(SP_TP, None),
        P(),
        P(),
        P(SP_TP),
        P(SP_TP, None),
        P(SP_TP, None),
        P("sp", None, TP),
        P("sp", None, TP),
        P("sp", TP, None),
    )

    return jax.shard_map(
        per_device, mesh=torus, in_specs=placed, out_specs=P(SP_TP, None), check_vma=False
    )
```
